512 devices in a mesh: rep: 2 (over z_hi), fs: 32 (over z_lo, y), tp: 8 (over x, core).
Axes of the slice: x: 4, y: 4, z: 16 (z_hi: 2, z_lo: 8; z = z_hi * 8 + z_lo), core: 2. Of those that a mesh axis runs over, the one named last changes fastest.
Arguments:
- inputs: bfloat16 [8192, 2048], P(('rep', 'fs'), 'tp'), may hold values from -6 to 6
- cotangent: bfloat16 [8192, 2048], P(('rep', 'fs'), 'tp'), may hold values from -8 to 8
- gate_weight: bfloat16 [2048, 2816], P('fs', 'tp'), may hold values from -0.125 to 0.125
- up_weight: bfloat16 [2048, 2816], P('fs', 'tp'), may hold values from -0.125 to 0.125
- down_weight: bfloat16 [2816, 2048], P('tp', 'fs'), may hold values from -0.109375 to 0.109375
Outputs:
- grad_inputs: bfloat16 [8192, 2048], P(('rep', 'fs'), 'tp')
- grad_gate_weight: float32 [2048, 2816], P('fs', 'tp')
- grad_up_weight: float32 [2048, 2816], P('fs', 'tp')
- grad_down_weight: float32 [2816, 2048], P('tp', 'fs')
The draws below stay inside these ranges and needn't reach their ends.
All inputs are finite; a program needn't handle non-finite values.
Results may differ from the reference program's by a relative error of at most 0.014.
Values may be sent and summed in bfloat16 or wider, within the bound.
No kernel may reach another device: no remote copies, remote signals or barrier semaphores. Data moves between devices by JAX's collectives and lax.ppermute only.
A program may use at most 64 MiB of HBM per device.

```python
import jax
import jax.numpy as jnp
from jax import lax

D = 2048
FF = 2816
TOKENS = 8192
N_TP = 8


def strengthened(result, rng, source, target, blocks, factor):
    def block_of(position):
        return (jnp.arange(result.shape[position]) // (result.shape[position] // blocks)).reshape((-1,) + (1,) * (result.ndim - 1 - position))

    one_side = jax.random.permutation(rng, blocks)[block_of(target)]
    other_side = (block_of(target) + blocks // 2) % blocks
    return jnp.where((block_of(source) == one_side) | (block_of(source) == other_side), factor * result, result)


def block_scale(rng, shape, split, least, top_value):
    def one(axis_at, shards_of):
        steps = jax.random.uniform(jax.random.fold_in(jax.random.fold_in(rng, 6), axis_at), (shards_of,), jnp.float32, least / len(split), top_value / len(split))
        return jnp.repeat(jnp.exp(steps), shape[axis_at] // shards_of).reshape((-1,) + (1,) * (len(shape) - axis_at - 1))

    loudness = one(*split[0])
    for cut in split[1:]:
        loudness = loudness * one(*cut)
    return loudness


def noise(stream_key, extent, deviation, reach, shards=(), kind=jnp.bfloat16):
    drawn = deviation * jax.random.normal(stream_key, extent, jnp.float32)
    if shards:
        drawn = drawn * block_scale(stream_key, extent, shards, -0.22, 0.18)
    return jnp.clip(drawn, -reach, reach).astype(kind)


def gaussian_with(own_key, extent, spread, bound, shards, heavy, held_as=jnp.bfloat16):
    drawn = spread * jax.random.normal(own_key, extent, jnp.float32)
    if shards:
        drawn = drawn * block_scale(own_key, extent, shards, -0.22, 0.18)
    return jnp.clip(strengthened(drawn, jax.random.fold_in(own_key, 3), *heavy), -bound, bound).astype(held_as)


def setup_inputs(seed: int = 0) -> dict:
    streams_of = jax.random.split(jax.random.key(seed), 6)
    return {
        "inputs": noise(streams_of[0], (TOKENS, D), 1.0, 6.0, ((0, 64), (1, 8))),
        "cotangent": gaussian_with(streams_of[1], (TOKENS, D), 1.0, 8.0, ((0, 64), (1, 8)), (0, 1, 64, 4.0)),
        "gate_weight": noise(streams_of[2], (D, FF), D ** -0.5, 0.125, ((0, 32), (1, 8))),
        "up_weight": noise(streams_of[3], (D, FF), D ** -0.5, 0.125, ((0, 32), (1, 8))),
        "down_weight": noise(streams_of[4], (FF, D), FF ** -0.5, 0.109375, ((0, 8), (1, 32))),
    }


def reference(inputs, cotangent, gate_weight, up_weight, down_weight):
    gate_pre = jnp.dot(inputs, gate_weight, preferred_element_type=jnp.float32)
    up_pre = jnp.dot(inputs, up_weight, preferred_element_type=jnp.float32)
    sigmoid_gate = jax.nn.sigmoid(gate_pre)
    activated = gate_pre * sigmoid_gate
    hidden = (activated * up_pre).astype(jnp.bfloat16)
    grad_hidden = jnp.dot(cotangent, down_weight.T, preferred_element_type=jnp.float32)
    grad_gate = (grad_hidden * up_pre * sigmoid_gate * (1.0 + gate_pre * (1.0 - sigmoid_gate))).astype(jnp.bfloat16)
    grad_up = (grad_hidden * activated).astype(jnp.bfloat16)
    grad_down_weight = jnp.dot(hidden.T, cotangent, preferred_element_type=jnp.float32)
    grad_gate_weight = jnp.dot(inputs.T, grad_gate, preferred_element_type=jnp.float32)
    grad_up_weight = jnp.dot(inputs.T, grad_up, preferred_element_type=jnp.float32)
    block_units = FF // N_TP
    running = jnp.zeros(inputs.shape, jnp.float32)
    for index in range(N_TP):
        lower = index * block_units
        upper = lower + block_units
        partial_sum = jnp.dot(grad_gate[:, lower:upper], gate_weight[:, lower:upper].T, preferred_element_type=jnp.float32)
        partial_sum = partial_sum + jnp.dot(grad_up[:, lower:upper], up_weight[:, lower:upper].T, preferred_element_type=jnp.float32)
        rounded = lax.optimization_barrier(partial_sum.astype(jnp.bfloat16))
        running = running + rounded.astype(jnp.float32)
    grad_inputs = running.astype(jnp.bfloat16)
    return (grad_inputs, grad_gate_weight, grad_up_weight, grad_down_weight)
```

```python
import jax
import jax.numpy as jnp
from jax import lax
from jax.experimental import pallas as pl
from jax.experimental.pallas import tpu as pltpu
from jax.sharding import Mesh, PartitionSpec as P


BF = jnp.bfloat16
F32 = jnp.float32
NZ, NZL, NY, NX, NC = 16, 8, 4, 4, 2
Z = ("zh", "zl")
PLANE = ("y", "x", "c")
SHIFTS = (0, 1, -1, 2, -2, 3, -3)
CUT = 128


def to_z(value, k):
    return lax.ppermute(value, Z, [(i, (i + k) % NZ) for i in range(NZ)])


def from_z(value, k):
    return to_z(value, -k)


def other_core(value):
    return lax.ppermute(value, "c", [(0, 1), (1, 0)])


def in_plane(value, k, x_core):
    pairs = []
    for y in range(NY):
        for x in range(NX):
            for c in range(NC):
                ty, tx = (y, (x + k) % NX) if c == x_core else ((y + k) % NY, x)
                pairs.append(((y * NX + x) * NC + c, (ty * NX + tx) * NC + c))
    return lax.ppermute(value, PLANE, pairs)


def dot(a, b, dims):
    return lax.dot_general(a, b, (dims, ((), ())), preferred_element_type=F32)


NN = ((1,), (0,))
NT = ((1,), (1,))


def layer_body(mine, other, w_refs, w_up, w_down, keep, send, outs, out_up, out_down):
    core = lax.axis_index("c")
    zl = lax.axis_index("zl")
    x = lax.axis_index("x")
    hid = w_refs[0].shape[0] // 3

    def where_of(k):
        t = (zl + k + NZL) % NZL
        return (t // NC + NX - x) % NX, t % NC

    def weights(i):
        if i < len(SHIFTS):
            return w_refs[i][: 2 * hid, :], w_refs[i][2 * hid :, :]
        return (
            jnp.concatenate([w_up[...], w_down[: 2 * hid - CUT, :]], axis=0),
            w_down[2 * hid - CUT :, :],
        )

    def run(inputs, cotan, flip):
        def tokens(ref, a, jx, c, d):
            part = ref[:, jx, c] if d == 0 else ref[jx, :, c]
            return part.reshape(NY * part.shape[1], part.shape[2])

        places = [where_of(k) for k in SHIFTS + (4,)]
        pre = None
        hid_grad = None
        for i, (jx, c) in enumerate(places):
            wgu, wd = weights(i)
            p = dot(wgu, tokens(inputs, 0, jx, c, 0), NT)
            q = dot(wd, tokens(cotan, 0, jx, 1 - c, 1), NT)
            pre = p if pre is None else pre + p
            hid_grad = q if hid_grad is None else hid_grad + q
        gate = pre[:hid]
        up = pre[hid:]
        sig = jax.nn.sigmoid(gate)
        act = gate * sig
        hidden = (act * up).astype(BF)
        g_gate = hid_grad * up * sig * (1.0 + gate * (1.0 - sig))
        g_up = hid_grad * act
        g_both = jnp.concatenate([g_gate, g_up], axis=0)
        g_turned = g_both.T.astype(BF)
        g_both = g_both.astype(BF)
        for i, (jx, c) in enumerate(places):
            wgu, _ = weights(i)
            pw = dot(g_both, tokens(inputs, 0, jx, c, 0), NN).astype(BF)
            pd = dot(hidden, tokens(cotan, 0, jx, 1 - c, 1), NN).astype(BF)
            if i < len(SHIFTS):
                outs[i][: 2 * hid, :] = pw
                outs[i][2 * hid :, :] = pd
            else:
                out_up[...] = pw[:CUT]
                out_down[: 2 * hid - CUT, :] = pw[CUT:]
                out_down[2 * hid - CUT :, :] = pd
            gi = dot(g_turned, wgu, NN).astype(BF)
            rows = gi.shape[0] // NY

            def put(ref, x_first):
                for jy in range(NY):
                    piece = gi[jy * rows : (jy + 1) * rows]
                    if x_first:
                        ref[jx, jy] = piece
                    else:
                        ref[jy, jx] = piece

            @pl.when(c == flip)
            def _():
                put(keep, flip == 0)

            @pl.when(c != flip)
            def _():
                put(send, flip == 1)

    @pl.when(core == 0)
    def _():
        run(mine, other, 0)

    @pl.when(core == 1)
    def _():
        run(other, mine, 1)


def layer(mine, other, ws, w_up, w_down):
    n = len(SHIFTS)

    def body(*refs):
        m, o = refs[:2]
        wr = refs[2 : 2 + n]
        wu, wd = refs[2 + n : 4 + n]
        keep, send = refs[4 + n : 6 + n]
        outs = refs[6 + n : 6 + 2 * n]
        ou, od = refs[6 + 2 * n :]
        layer_body(m, o, wr, wu, wd, keep, send, outs, ou, od)

    rows, cols = mine.shape[3:]
    S = jax.ShapeDtypeStruct
    shapes = [S((4, 4, rows, cols), BF)] * 2 + [S(w.shape, BF) for w in (*ws, w_up, w_down)]
    vm = pl.BlockSpec(memory_space=pltpu.VMEM)
    res = pl.pallas_call(
        body,
        in_specs=[vm] * (4 + n),
        out_specs=[vm] * len(shapes),
        out_shape=shapes,
        name="layer",
    )(mine, other, *ws, w_up, w_down)
    return res[0], res[1], res[2 : 2 + n], res[2 + n], res[3 + n]


def per_device(inputs, cotangent, gate_weight, up_weight, down_weight):
    core = lax.axis_index("c")
    first = core == 0
    hid = gate_weight.shape[1] // NY
    rows_d = gate_weight.shape[0]

    kept = jnp.where(first, inputs, cotangent)
    given = jnp.where(first, cotangent, inputs)
    block = jnp.stack([kept, other_core(given)])

    def cut(w):
        return w.reshape(NY, hid, rows_d)

    packed = jnp.concatenate([cut(gate_weight.T), cut(up_weight.T), cut(down_weight)], axis=1)
    w_own = lax.all_to_all(packed, "y", 0, 0, tiled=True)
    w_own = jnp.moveaxis(w_own, 0, 1).reshape(3 * hid, NY * rows_d)

    ws = [w_own] + [from_z(w_own, k) for k in SHIFTS[1:]]
    w_up = from_z(w_own[:CUT], 4)
    w_down = from_z(w_own[CUT:], -4)

    line = jnp.stack([block] + [in_plane(block, -k, 0) for k in (1, 2, 3)])
    mine = jnp.stack([line] + [in_plane(line, -k, 1) for k in (1, 2, 3)])
    other = other_core(mine)

    keep, send, outs, out_up, out_down = layer(mine, other, ws, w_up, w_down)

    arrived = [outs[0]] + [to_z(o, k) for o, k in zip(outs[1:], SHIFTS[1:])]
    far = jnp.concatenate([to_z(out_up, 4), to_z(out_down, -4)], axis=0)
    total = far.astype(F32)
    for a in arrived:
        total = total + a.astype(F32)
    total = total.astype(BF)
    partner = lax.ppermute(total, "zh", [(0, 1), (1, 0)])
    total = total.astype(F32) + partner.astype(F32)
    total = jnp.moveaxis(total.reshape(3 * hid, NY, rows_d), 1, 0)
    total = lax.all_to_all(total, "y", 0, 0, tiled=True)
    g_gate = total[:, :hid].reshape(NY * hid, rows_d).T
    g_up = total[:, hid : 2 * hid].reshape(NY * hid, rows_d).T
    g_down = total[:, 2 * hid :].reshape(NY * hid, rows_d)

    chip = keep.astype(F32) + other_core(send).astype(F32)
    part = chip[0].astype(BF).astype(F32)
    for k in (1, 2, 3):
        part = part + in_plane(chip[k].astype(BF), k, 0).astype(F32)
    done = part[0]
    for k in (1, 2, 3):
        done = done + in_plane(part[k].astype(BF), k, 1).astype(F32)
    return (done.astype(BF), g_gate, g_up, g_down)


def solution(mesh):
    fine = Mesh(mesh.devices.reshape(2, NZL, NY, NX, NC), ("zh", "zl", "y", "x", "c"))
    tok, fs, tp = ("zh", "zl", "y"), ("zl", "y"), ("x", "c")
    return jax.shard_map(
        per_device,
        mesh=fine,
        in_specs=(P(tok, tp), P(tok, tp), P(fs, tp), P(fs, tp), P(tp, fs)),
        out_specs=(P(tok, tp), P(fs, tp), P(fs, tp), P(tp, fs)),
        check_vma=False,
    )
```

```python
import jax
import jax.numpy as jnp
from jax import lax
from jax.experimental import pallas as pl
from jax.experimental.pallas import tpu as pltpu
from jax.sharding import Mesh, PartitionSpec as P


BF = jnp.bfloat16
F32 = jnp.float32
NR, NY, NX, NC = 4, 4, 4, 2
PLANE = ("y", "x", "c")
QUADS = ("zh", "zq")
VM = pl.BlockSpec(memory_space=pltpu.VMEM)
NN = ((1,), (0,))
NT = ((1,), (1,))


def swapped(value, axis):
    return lax.ppermute(value, axis, [(0, 1), (1, 0)])


def moved(value, k, x_core):
    pairs = []
    for y in range(NY):
        for x in range(NX):
            for c in range(NC):
                ty, tx = (y, (x + k) % NX) if c == x_core else ((y + k) % NY, x)
                pairs.append(((y * NX + x) * NC + c, (ty * NX + tx) * NC + c))
    return lax.ppermute(value, PLANE, pairs)


def line_gather(value, x_core):
    return jnp.stack([value] + [moved(value, -k, x_core) for k in (1, 2, 3)])


def line_sum(value, x_core):
    total = value[0].astype(F32)
    for k in (1, 2, 3):
        total = total + moved(value[k], k, x_core).astype(F32)
    return total.astype(BF)


def dot(a, b, dims):
    return lax.dot_general(a, b, (dims, ((), ())), preferred_element_type=F32)


def sides(a, b):
    return jnp.concatenate([a, b], axis=1)


def call(body, args, shapes, scratch=(), mib=8):
    single = not isinstance(shapes, (list, tuple))
    return pl.pallas_call(
        body,
        in_specs=[VM] * len(args),
        out_specs=VM if single else [VM] * len(shapes),
        out_shape=shapes,
        scratch_shapes=scratch,
        compiler_params=pltpu.CompilerParams(vmem_limit_bytes=mib * 2**20),
    )(*args)


def pack_body(wg, wu, wd, out):
    hid = wd.shape[1] // NY
    tg = wg[...].astype(F32).T
    tu = wu[...].astype(F32).T
    td = wd[...].astype(F32).T
    parts = []
    for y in range(NY):
        s = slice(y * hid, (y + 1) * hid)
        parts.append(jnp.concatenate([tg[s], tu[s], td[s]], axis=0))
    out[0] = sides(parts[0], parts[2]).astype(BF)
    out[1] = sides(parts[1], parts[3]).astype(BF)


def spread_body(own, far, out):
    half = own.shape[2] // 2
    for i in range(2):
        o, f = own[i].astype(F32), far[i].astype(F32)
        low = sides(o[:, :half], f[:, :half]).astype(BF)
        high = sides(o[:, half:], f[:, half:]).astype(BF)
        for r in range(NR):
            out[r * NY + i] = low
            out[r * NY + i + 2] = high


def layer_body(mine, other, chunks, keep, send, pieces, wt):
    core = lax.axis_index("c")
    zq = lax.axis_index("zq")
    x_here = lax.axis_index("x")
    hid = chunks.shape[1] // 3
    half = chunks.shape[2] // 2

    def x_of(side, r):
        return (2 * (zq if side == 0 else 1 - zq) + r // NC + NX - x_here) % NX

    for r in range(NR):
        for side in range(2):
            cut = slice(side * half, (side + 1) * half)
            wt[2 * r + side] = jnp.concatenate(
                [chunks[r * NY + y][:, cut] for y in range(NY)], axis=1
            )

    def run(inputs, cotan, me):
        def tokens(part):
            return part.reshape(NY * part.shape[1], part.shape[2])

        def in_block(side, r):
            return tokens(inputs[:, x_of(side, r), r % NC])

        def co_block(side, r):
            return tokens(cotan[x_of(side, r), :, 1 - r % NC])

        pre = None
        hid_grad = None
        for r in range(NR):
            for side in range(2):
                p = dot(wt[2 * r + side, : 2 * hid, :], in_block(side, r), NT)
                q = dot(wt[2 * r + side, 2 * hid :, :], co_block(side, r), NT)
                pre = p if pre is None else pre + p
                hid_grad = q if hid_grad is None else hid_grad + q
        gate = pre[:hid]
        up = pre[hid:]
        sig = jax.nn.sigmoid(gate)
        act = gate * sig
        hidden = (act * up).astype(BF)
        g_gate = hid_grad * up * sig * (1.0 + gate * (1.0 - sig))
        g_up = hid_grad * act
        g_both = jnp.concatenate([g_gate, g_up], axis=0)
        g_turned = g_both.T.astype(BF)
        g_both = g_both.astype(BF)
        for r in range(NR):
            made = []
            for side in range(2):
                pw = dot(g_both, in_block(side, r), NN)
                pd = dot(hidden, co_block(side, r), NN)
                made.append(jnp.concatenate([pw, pd], axis=0))
                gi = dot(g_turned, wt[2 * r + side, : 2 * hid, :], NN).astype(BF)
                rows = gi.shape[0] // NY
                x = x_of(side, r)
                ref = keep if r % NC == me else send
                x_first = (r % NC) == 0
                for y in range(NY):
                    piece = gi[y * rows : (y + 1) * rows]
                    if x_first:
                        ref[x, y] = piece
                    else:
                        ref[y, x] = piece
            for y in range(NY):
                s = slice(y * half, (y + 1) * half)
                pieces[r * NY + y] = sides(made[0][:, s], made[1][:, s]).astype(BF)

    @pl.when(core == 0)
    def _():
        run(mine, other, 0)

    @pl.when(core == 1)
    def _():
        run(other, mine, 1)


def quad_body(pieces, out):
    zq = lax.axis_index("zq")
    half = pieces.shape[2] // 2

    def total(y):
        s = pieces[y].astype(F32)
        for r in range(1, NR):
            s = s + pieces[r * NY + y].astype(F32)
        return s

    for i in range(2):
        low, high = total(i), total(i + 2)
        own = sides(low[:, :half], high[:, :half]).astype(BF)
        far = sides(low[:, half:], high[:, half:]).astype(BF)
        for h in range(2):
            out[2 * h + zq, i] = own
            out[2 * h + 1 - zq, i] = far


def last_body(parts, gg, gu, gd):
    hid = parts.shape[2] // 3
    half = parts.shape[3] // 2
    s = []
    for i in range(2):
        v = parts[0, i].astype(F32)
        for q in range(1, 4):
            v = v + parts[q, i].astype(F32)
        s.append(v)
    by_y = [s[0][:, :half], s[1][:, :half], s[0][:, half:], s[1][:, half:]]
    gg[...] = jnp.concatenate([b[:hid] for b in by_y], axis=0).T
    gu[...] = jnp.concatenate([b[hid : 2 * hid] for b in by_y], axis=0).T
    gd[...] = jnp.concatenate([b[2 * hid :] for b in by_y], axis=0).T


def per_device(inputs, cotangent, gate_weight, up_weight, down_weight):
    S = jax.ShapeDtypeStruct
    rows_d, ff = gate_weight.shape
    hid = ff // NY
    rows, cols = inputs.shape

    first = lax.axis_index("c") == 0
    kept = jnp.where(first, inputs, cotangent)
    given = jnp.where(first, cotangent, inputs)
    got = swapped(given, "c")
    block = jnp.stack([kept, got])

    packed = call(pack_body, (gate_weight, up_weight, down_weight.T), S((2, 3 * hid, 2 * rows_d), BF))
    far = swapped(packed, "zq")
    chunks = call(spread_body, (packed, far), S((NR * NY, 3 * hid, 2 * rows_d), BF))
    chunks = lax.all_to_all(chunks, ("zr", "y"), 0, 0, tiled=True)

    line = line_gather(block, 0)
    mine = line_gather(line, 1)
    other = swapped(mine, "c")

    tiles = S((4, 4, rows, cols), BF)
    keep, send, pieces = call(
        layer_body,
        (mine, other, chunks),
        [tiles, tiles, S(chunks.shape, BF)],
        [pltpu.VMEM((2 * NR, 3 * hid, NY * rows_d), BF)],
        28,
    )

    pieces = lax.all_to_all(pieces, ("zr", "y"), 0, 0, tiled=True)
    quads = call(quad_body, (pieces,), S((4, 2, 3 * hid, 2 * rows_d), BF))
    quads = lax.all_to_all(quads, QUADS, 0, 0, tiled=True)
    g_gate, g_up, g_down = call(
        last_body,
        (quads,),
        [S((rows_d, ff), F32), S((rows_d, ff), F32), S((rows_d, ff), F32)],
    )

    theirs = swapped(send, "c")
    chip = (keep.astype(F32) + theirs.astype(F32)).astype(BF)
    part = line_sum(chip, 0)
    done = line_sum(part, 1)
    return (done, g_gate, g_up, g_down.T)


def solution(mesh):
    fine = Mesh(mesh.devices.reshape(2, 2, NR, NY, NX, NC), ("zh", "zq", "zr", "y", "x", "c"))
    tok, fs, tp = ("zh", "zq", "zr", "y"), ("zq", "zr", "y"), ("x", "c")

    return jax.shard_map(
        per_device,
        mesh=fine,
        in_specs=(P(tok, tp), P(tok, tp), P(fs, tp), P(fs, tp), P(tp, fs)),
        out_specs=(P(tok, tp), P(fs, tp), P(fs, tp), P(tp, fs)),
        check_vma=False,
    )
```

```python
import jax
import jax.numpy as jnp
from jax import lax
from jax.experimental import pallas as pl
from jax.experimental.pallas import tpu as pltpu
from jax.sharding import Mesh, PartitionSpec as P


BF = jnp.bfloat16
F32 = jnp.float32
NQ, NR, NY, NX, NC = 2, 4, 4, 4, 2
PLANE = ("y", "x", "c")
VM = pl.BlockSpec(memory_space=pltpu.VMEM)
NN = ((1,), (0,))
NT = ((1,), (1,))


def swapped(value):
    return lax.ppermute(value, "c", [(0, 1), (1, 0)])


def moved(value, k, x_core):
    pairs = []
    for y in range(NY):
        for x in range(NX):
            for c in range(NC):
                ty, tx = (y, (x + k) % NX) if c == x_core else ((y + k) % NY, x)
                pairs.append(((y * NX + x) * NC + c, (ty * NX + tx) * NC + c))
    return lax.ppermute(value, PLANE, pairs)


def line_gather(value, x_core):
    return [value] + [moved(value, -k, x_core) for k in (1, 2, 3)]


def line_sum(value, x_core):
    total = value[0].astype(F32)
    for k in (1, 2, 3):
        total = total + moved(value[k], k, x_core).astype(F32)
    return total.astype(BF)


def dot(a, b, dims):
    return lax.dot_general(a, b, (dims, ((), ())), preferred_element_type=F32)


def call(body, args, shapes, mib=8, far_in=0, far_out=False):
    single = not isinstance(shapes, (list, tuple))
    shapes = [shapes] if single else list(shapes)
    n, m = len(args), len(shapes)
    loads, stores = far_in, m if far_out else 0

    def whole(*refs):
        ins, outs, rest = list(refs[:n]), list(refs[n : n + m]), refs[n + m :]
        near_in, near_out = rest[:loads], rest[loads : loads + stores]
        if loads:
            sems = rest[loads + stores]
            copies = [pltpu.make_async_copy(ins[i], near_in[i], sems.at[i]) for i in range(loads)]
            for c in copies:
                c.start()
            for c in copies:
                c.wait()
        body(*near_in, *ins[loads:], *(near_out if stores else outs))
        if stores:
            sems = rest[-1]
            copies = [pltpu.make_async_copy(near_out[i], outs[i], sems.at[i]) for i in range(m)]
            for c in copies:
                c.start()
            for c in copies:
                c.wait()

    far = pl.BlockSpec(memory_space=pltpu.HBM)
    scratch = [pltpu.VMEM(a.shape, a.dtype) for a in args[:loads]]
    scratch += [pltpu.VMEM(a.shape, a.dtype) for a in shapes[:stores]]
    scratch += [pltpu.SemaphoreType.DMA((k,)) for k in (loads, stores) if k]
    out = pl.pallas_call(
        whole,
        in_specs=[far] * loads + [VM] * (n - loads),
        out_specs=[far if far_out else VM] * m,
        out_shape=shapes,
        scratch_shapes=scratch,
        compiler_params=pltpu.CompilerParams(vmem_limit_bytes=mib * 2**20),
    )(*args)
    return out[0] if single else out


def folded(value, cut):
    low = value[cut:]
    gap = jnp.zeros((2 * cut - value.shape[0], value.shape[1]), value.dtype)
    return jnp.concatenate([value[:cut], jnp.concatenate([low, gap], axis=0)], axis=1)


def unfolded(value, n):
    cut, width = value.shape
    return jnp.concatenate([value[:, : width // 2], value[: n - cut, width // 2 :]], axis=0)


def cut_of(n):
    return -(-n // 16) * 8


def pack_body(wg, wu, wd, out):
    hid = wd.shape[1] // NY
    tg = wg[...].astype(F32).T
    tu = wu[...].astype(F32).T
    td = wd[...].astype(F32).T
    for y in range(NY):
        s = slice(y * hid, (y + 1) * hid)
        part = jnp.concatenate([tg[s], tu[s], td[s]], axis=0)
        part = folded(part, out.shape[1]).astype(BF)
        for q in range(NQ):
            out[q * NY + y] = part


def spread_body(parts, out):
    n = out.shape[1]
    whole = jnp.concatenate(
        [unfolded(parts[i].astype(F32), n).astype(BF) for i in range(NQ * NY)], axis=1
    )
    for r in range(NR):
        out[r] = whole


def layer_body(mine, other, chunks, keep, send, pieces):
    core = lax.axis_index("c")
    x_here = lax.axis_index("x")
    hid = chunks.shape[1] // 3
    width = chunks.shape[2] // NQ

    def run(inputs, cotan, me):
        def in_block(k, c):
            return jnp.concatenate([inputs[j][k, c] for j in range(NY)], axis=0)

        def co_block(k, c):
            part = cotan[k][:, 1 - c]
            return part.reshape(NY * part.shape[1], part.shape[2])

        def place(k, c):
            x = (x_here + k) % NX
            return (x % 2) * NC + c, pl.ds(pl.multiple_of((x // 2) * width, width), width)

        blocks = [(k, c) for k in range(NX) for c in range(NC)]
        pre = None
        hid_grad = None
        for k, c in blocks:
            r, s = place(k, c)
            p = dot(chunks[r, : 2 * hid, s], in_block(k, c), NT)
            q = dot(chunks[r, 2 * hid :, s], co_block(k, c), NT)
            pre = p if pre is None else pre + p
            hid_grad = q if hid_grad is None else hid_grad + q
        gate = pre[:hid]
        up = pre[hid:]
        sig = jax.nn.sigmoid(gate)
        act = gate * sig
        hidden = (act * up).astype(BF)
        g_gate = hid_grad * up * sig * (1.0 + gate * (1.0 - sig))
        g_up = hid_grad * act
        g_both = jnp.concatenate([g_gate, g_up], axis=0)
        g_turned = g_both.T.astype(BF)
        g_both = g_both.astype(BF)
        for k, c in blocks:
            r, s = place(k, c)
            pieces[r, : 2 * hid, s] = dot(g_both, in_block(k, c), NN).astype(BF)
            pieces[r, 2 * hid :, s] = dot(hidden, co_block(k, c), NN).astype(BF)
            gi = dot(g_turned, chunks[r, : 2 * hid, s], NN).astype(BF)
            rows = gi.shape[0] // NY
            ref = keep if c == me else send
            for j in range(NY):
                piece = gi[j * rows : (j + 1) * rows]
                if c == 0:
                    ref[k, j] = piece
                else:
                    ref[j, k] = piece

    @pl.when(core == 0)
    def _():
        run(mine, other, 0)

    @pl.when(core == 1)
    def _():
        run(other, mine, 1)


def sum_body(pieces, out):
    total = pieces[0].astype(F32)
    for r in range(1, NR):
        total = total + pieces[r].astype(F32)
    width = total.shape[1] // (NQ * NY)
    for i in range(NQ * NY):
        part = folded(total[:, i * width : (i + 1) * width], out.shape[1]).astype(BF)
        for h in range(2):
            out[h * NQ * NY + i] = part


def last_body(parts, gg, gu, gd):
    hid = gg.shape[1] // NY
    by_y = []
    for y in range(NY):
        v = parts[y].astype(F32)
        for q in range(1, 4):
            v = v + parts[q * NY + y].astype(F32)
        by_y.append(unfolded(v, 3 * hid))
    gg[...] = jnp.concatenate([b[:hid] for b in by_y], axis=0).T
    gu[...] = jnp.concatenate([b[hid : 2 * hid] for b in by_y], axis=0).T
    gd[...] = jnp.concatenate([b[2 * hid :] for b in by_y], axis=0).T


def per_device(inputs, cotangent, gate_weight, up_weight, down_weight):
    S = jax.ShapeDtypeStruct
    rows_d, ff = gate_weight.shape
    hid = ff // NY
    cut = cut_of(3 * hid)
    rows, cols = inputs.shape

    first = lax.axis_index("c") == 0
    kept = jnp.where(first, inputs, cotangent)
    given = jnp.where(first, cotangent, inputs)
    got = swapped(given)
    block = jnp.stack([kept, got])

    packed = call(
        pack_body,
        (gate_weight, up_weight, down_weight.T),
        S((NQ * NY, cut, 2 * rows_d), BF),
        far_in=3,
    )
    packed = lax.all_to_all(packed, ("zq", "y"), 0, 0, tiled=True)
    chunks = call(spread_body, (packed,), S((NR, 3 * hid, NQ * NY * rows_d), BF))
    chunks = lax.all_to_all(chunks, "zr", 0, 0, tiled=True)

    line = jnp.stack(line_gather(block, 0))
    mine = line_gather(line, 1)
    other = [swapped(m) for m in mine]

    tiles = S((4, 4, rows, cols), BF)

    def body(*refs):
        layer_body(refs[:4], refs[4:8], *refs[8:])

    keep, send, pieces = call(
        body,
        (*mine, *other, chunks),
        [tiles, tiles, S(chunks.shape, BF)],
        28,
        far_in=8,
        far_out=True,
    )

    pieces = lax.all_to_all(pieces, "zr", 0, 0, tiled=True)
    ring = call(sum_body, (pieces,), S((2 * NQ * NY, cut, 2 * rows_d), BF))
    ring = lax.all_to_all(ring, ("zh", "zq", "y"), 0, 0, tiled=True)
    g_gate, g_up, g_down = call(last_body, (ring,), [S((rows_d, ff), F32)] * 3)

    theirs = swapped(send)
    chip = (keep.astype(F32) + theirs.astype(F32)).astype(BF)
    part = line_sum(chip, 0)
    done = line_sum(part, 1)
    return (done, g_gate, g_up, g_down.T)


def solution(mesh):
    fine = Mesh(mesh.devices.reshape(2, NQ, NR, NY, NX, NC), ("zh", "zq", "zr", "y", "x", "c"))
    tok, fs, tp = ("zh", "zq", "zr", "y"), ("zq", "zr", "y"), ("x", "c")

    return jax.shard_map(
        per_device,
        mesh=fine,
        in_specs=(P(tok, tp), P(tok, tp), P(fs, tp), P(fs, tp), P(tp, fs)),
        out_specs=(P(tok, tp), P(fs, tp), P(fs, tp), P(tp, fs)),
        check_vma=False,
    )
```

```python
import jax
import jax.numpy as jnp
from jax import lax
from jax.experimental import pallas as pl
from jax.experimental.pallas import tpu as pltpu
from jax.sharding import Mesh, PartitionSpec as P


BF = jnp.bfloat16
F32 = jnp.float32
NQ, NR, NY, NX, NC = 2, 4, 4, 4, 2
PLANE = ("y", "x", "c")
VM = pl.BlockSpec(memory_space=pltpu.VMEM)
NN = ((1,), (0,))
NT = ((1,), (1,))


def swapped(value):
    return lax.ppermute(value, "c", [(0, 1), (1, 0)])


def moved(value, k, x_core):
    pairs = []
    for y in range(NY):
        for x in range(NX):
            for c in range(NC):
                ty, tx = (y, (x + k) % NX) if c == x_core else ((y + k) % NY, x)
                pairs.append(((y * NX + x) * NC + c, (ty * NX + tx) * NC + c))
    return lax.ppermute(value, PLANE, pairs)


def line_gather(value, x_core):
    return [value] + [moved(value, -k, x_core) for k in (1, 2, 3)]


def line_sum(value, x_core):
    total = value[0].astype(F32)
    for k in (1, 2, 3):
        total = total + moved(value[k], k, x_core).astype(F32)
    return total.astype(BF)


def dot(a, b, dims):
    return lax.dot_general(a, b, (dims, ((), ())), preferred_element_type=F32)


def call(body, args, shapes, mib=8, far_in=0, far_out=False, own=()):
    single = not isinstance(shapes, (list, tuple))
    shapes = [shapes] if single else list(shapes)
    n, m = len(args), len(shapes)
    loads, stores = far_in, m if far_out else 0

    def whole(*refs):
        ins, outs, rest = list(refs[:n]), list(refs[n : n + m]), refs[n + m :]
        mid = loads + stores
        near_in, near_out = rest[:loads], rest[loads:mid]
        held, rest = rest[mid : mid + len(own)], rest[mid + len(own) :]
        if loads:
            sems = rest[0]
            copies = [pltpu.make_async_copy(ins[i], near_in[i], sems.at[i]) for i in range(loads)]
            for c in copies:
                c.start()
            for c in copies:
                c.wait()
        body(*near_in, *ins[loads:], *(near_out if stores else outs), *held)
        if stores:
            sems = rest[-1]
            copies = [pltpu.make_async_copy(near_out[i], outs[i], sems.at[i]) for i in range(m)]
            for c in copies:
                c.start()
            for c in copies:
                c.wait()

    far = pl.BlockSpec(memory_space=pltpu.HBM)
    scratch = [pltpu.VMEM(a.shape, a.dtype) for a in args[:loads]]
    scratch += [pltpu.VMEM(a.shape, a.dtype) for a in shapes[:stores]]
    scratch += list(own)
    scratch += [pltpu.SemaphoreType.DMA((k,)) for k in (loads, stores) if k]
    out = pl.pallas_call(
        whole,
        in_specs=[far] * loads + [VM] * (n - loads),
        out_specs=[far if far_out else VM] * m,
        out_shape=shapes,
        scratch_shapes=scratch,
        compiler_params=pltpu.CompilerParams(vmem_limit_bytes=mib * 2**20),
    )(*args)
    return out[0] if single else out


def sides(a, b):
    return jnp.concatenate([a, b], axis=1)


def pack_body(wg, wu, wd, out):
    hid = wd.shape[1] // NY
    tg = wg[...].astype(F32).T
    tu = wu[...].astype(F32).T
    td = wd[...].astype(F32).T
    parts = []
    for y in range(NY):
        s = slice(y * hid, (y + 1) * hid)
        parts.append(jnp.concatenate([tg[s], tu[s], td[s]], axis=0))
    out[0] = sides(parts[0], parts[2]).astype(BF)
    out[1] = sides(parts[1], parts[3]).astype(BF)


def spread_body(own, far, out):
    half = own.shape[2] // 2
    for i in range(2):
        o, f = own[i].astype(F32), far[i].astype(F32)
        low = sides(o[:, :half], f[:, :half]).astype(BF)
        high = sides(o[:, half:], f[:, half:]).astype(BF)
        for r in range(NR):
            out[r * NY + i] = low
            out[r * NY + i + 2] = high


def layer_body(mine, other, chunks, keep, send, pieces, wt, made):
    core = lax.axis_index("c")
    x_here = lax.axis_index("x")
    zq = lax.axis_index("zq")
    hid = chunks.shape[1] // 3
    half = chunks.shape[2] // 2

    for r in range(NR):
        for side in range(NQ):
            cut = slice(side * half, (side + 1) * half)
            wt[NQ * r + side] = jnp.concatenate(
                [chunks[r * NY + y][:, cut] for y in range(NY)], axis=1
            )

    def run(even, odd, me):
        def block(k, c, which):
            if c == 0:
                return jnp.concatenate([even[j][k, which] for j in range(NY)], axis=0)
            part = odd[k][:, which]
            return part.reshape(NY * part.shape[1], part.shape[2])

        def place(k, c):
            x = (x_here + k) % NX
            return NQ * ((x % 2) * NC + c) + (x // 2 + zq) % NQ

        blocks = [(k, c) for k in range(NX) for c in range(NC)]
        pre = None
        hid_grad = None
        for k, c in blocks:
            i = place(k, c)
            p = dot(wt[i, : 2 * hid, :], block(k, c, 0), NT)
            q = dot(wt[i, 2 * hid :, :], block(k, c, 1), NT)
            pre = p if pre is None else pre + p
            hid_grad = q if hid_grad is None else hid_grad + q
        gate = pre[:hid]
        up = pre[hid:]
        sig = jax.nn.sigmoid(gate)
        act = gate * sig
        hidden = (act * up).astype(BF)
        g_gate = hid_grad * up * sig * (1.0 + gate * (1.0 - sig))
        g_up = hid_grad * act
        g_both = jnp.concatenate([g_gate, g_up], axis=0)
        g_turned = g_both.T.astype(BF)
        g_both = g_both.astype(BF)
        for k, c in blocks:
            i = place(k, c)
            made[i, : 2 * hid, :] = dot(g_both, block(k, c, 0), NN).astype(BF)
            made[i, 2 * hid :, :] = dot(hidden, block(k, c, 1), NN).astype(BF)
            gi = dot(g_turned, wt[i, : 2 * hid, :], NN).astype(BF)
            rows = gi.shape[0] // NY
            ref = keep if c == me else send
            for j in range(NY):
                piece = gi[j * rows : (j + 1) * rows]
                if c == 0:
                    ref[k, j] = piece
                else:
                    ref[j, k] = piece

    @pl.when(core == 0)
    def _():
        run(mine, other, 0)

    @pl.when(core == 1)
    def _():
        run(other, mine, 1)

    for r in range(NR):
        for y in range(NY):
            s = slice(y * half, (y + 1) * half)
            pieces[r * NY + y] = sides(made[NQ * r, :, s], made[NQ * r + 1, :, s])


def sum_body(pieces, out):
    zq = lax.axis_index("zq")
    half = pieces.shape[2] // 2

    def total(y):
        s = pieces[y].astype(F32)
        for r in range(1, NR):
            s = s + pieces[r * NY + y].astype(F32)
        return s

    for i in range(2):
        low, high = total(i), total(i + 2)
        own = sides(low[:, :half], high[:, :half]).astype(BF)
        far = sides(low[:, half:], high[:, half:]).astype(BF)
        for h in range(2):
            out[2 * h + zq, i] = own
            out[2 * h + 1 - zq, i] = far


def last_body(parts, gg, gu, gd):
    hid = parts.shape[2] // 3
    half = parts.shape[3] // 2
    s = []
    for i in range(2):
        v = parts[0, i].astype(F32)
        for q in range(1, 4):
            v = v + parts[q, i].astype(F32)
        s.append(v)
    by_y = [s[0][:, :half], s[1][:, :half], s[0][:, half:], s[1][:, half:]]
    gg[...] = jnp.concatenate([b[:hid] for b in by_y], axis=0).T
    gu[...] = jnp.concatenate([b[hid : 2 * hid] for b in by_y], axis=0).T
    gd[...] = jnp.concatenate([b[2 * hid :] for b in by_y], axis=0).T


def per_device(inputs, cotangent, gate_weight, up_weight, down_weight):
    S = jax.ShapeDtypeStruct
    rows_d, ff = gate_weight.shape
    hid = ff // NY
    rows, cols = inputs.shape

    packed = call(
        pack_body,
        (gate_weight, up_weight, down_weight.T),
        S((2, 3 * hid, 2 * rows_d), BF),
        60,
        far_in=3,
    )
    far = lax.ppermute(packed, "zq", [(0, 1), (1, 0)])
    chunks = call(spread_body, (packed, far), S((NR * NY, 3 * hid, 2 * rows_d), BF))
    chunks = lax.all_to_all(chunks, ("zr", "y"), 0, 0, tiled=True)

    block = jnp.stack([inputs, cotangent])
    line = jnp.stack(line_gather(block, 0))
    mine = line_gather(line, 1)
    other = [swapped(m) for m in mine]

    tiles = S((4, 4, rows, cols), BF)

    def body(*refs):
        layer_body(refs[:4], refs[4:8], *refs[8:])

    blocks = pltpu.VMEM((NQ * NR, 3 * hid, NY * rows_d), BF)
    keep, send, pieces = call(
        body,
        (*mine, *other, chunks),
        [tiles, tiles, S(chunks.shape, BF)],
        60,
        far_in=9,
        far_out=True,
        own=[blocks, blocks],
    )

    pieces = lax.all_to_all(pieces, ("zr", "y"), 0, 0, tiled=True)
    ring = call(sum_body, (pieces,), S((4, 2, 3 * hid, 2 * rows_d), BF))
    ring = lax.all_to_all(ring, ("zh", "zq"), 0, 0, tiled=True)
    g_gate, g_up, g_down = call(last_body, (ring,), [S((rows_d, ff), F32)] * 3)

    theirs = swapped(send)
    chip = (keep.astype(F32) + theirs.astype(F32)).astype(BF)
    part = line_sum(chip, 0)
    done = line_sum(part, 1)
    return (done, g_gate, g_up, g_down.T)


def solution(mesh):
    fine = Mesh(mesh.devices.reshape(2, NQ, NR, NY, NX, NC), ("zh", "zq", "zr", "y", "x", "c"))
    tok, fs, tp = ("zh", "zq", "zr", "y"), ("zq", "zr", "y"), ("x", "c")

    return jax.shard_map(
        per_device,
        mesh=fine,
        in_specs=(P(tok, tp), P(tok, tp), P(fs, tp), P(fs, tp), P(tp, fs)),
        out_specs=(P(tok, tp), P(fs, tp), P(fs, tp), P(tp, fs)),
        check_vma=False,
    )
```

```python
import jax
import jax.numpy as jnp
from jax import lax
from jax.experimental import pallas as pl
from jax.experimental.pallas import tpu as pltpu
from jax.sharding import Mesh, PartitionSpec as P


BF = jnp.bfloat16
F32 = jnp.float32
NQ, NR, NY, NX, NC = 2, 4, 4, 4, 2
PLANE = ("y", "x", "c")
VM = pl.BlockSpec(memory_space=pltpu.VMEM)
NN = ((1,), (0,))
NT = ((1,), (1,))


def swapped(value):
    return lax.ppermute(value, "c", [(0, 1), (1, 0)])


def moved(value, k, x_core):
    pairs = []
    for y in range(NY):
        for x in range(NX):
            for c in range(NC):
                ty, tx = (y, (x + k) % NX) if c == x_core else ((y + k) % NY, x)
                pairs.append(((y * NX + x) * NC + c, (ty * NX + tx) * NC + c))
    return lax.ppermute(value, PLANE, pairs)


def line_gather(value, x_core):
    return [value] + [moved(value, -k, x_core) for k in (1, 2, 3)]


def line_sum(value, x_core):
    total = value[0].astype(F32)
    for k in (1, 2, 3):
        total = total + moved(value[k], k, x_core).astype(F32)
    return total.astype(BF)


def dot(a, b, dims):
    return lax.dot_general(a, b, (dims, ((), ())), preferred_element_type=F32)


def call(body, args, shapes, mib=8, far_in=0, far_out=False, own=()):
    single = not isinstance(shapes, (list, tuple))
    shapes = [shapes] if single else list(shapes)
    n, m = len(args), len(shapes)
    loads, stores = far_in, m if far_out else 0

    def whole(*refs):
        ins, outs, rest = list(refs[:n]), list(refs[n : n + m]), refs[n + m :]
        mid = loads + stores
        near_in, near_out = rest[:loads], rest[loads:mid]
        held, rest = rest[mid : mid + len(own)], rest[mid + len(own) :]
        if loads:
            sems = rest[0]
            copies = [pltpu.make_async_copy(ins[i], near_in[i], sems.at[i]) for i in range(loads)]
            for c in copies:
                c.start()
            for c in copies:
                c.wait()
        body(*near_in, *ins[loads:], *(near_out if stores else outs), *held)
        if stores:
            sems = rest[-1]
            copies = [pltpu.make_async_copy(near_out[i], outs[i], sems.at[i]) for i in range(m)]
            for c in copies:
                c.start()
            for c in copies:
                c.wait()

    far = pl.BlockSpec(memory_space=pltpu.HBM)
    scratch = [pltpu.VMEM(a.shape, a.dtype) for a in args[:loads]]
    scratch += [pltpu.VMEM(a.shape, a.dtype) for a in shapes[:stores]]
    scratch += list(own)
    scratch += [pltpu.SemaphoreType.DMA((k,)) for k in (loads, stores) if k]
    out = pl.pallas_call(
        whole,
        in_specs=[far] * loads + [VM] * (n - loads),
        out_specs=[far if far_out else VM] * m,
        out_shape=shapes,
        scratch_shapes=scratch,
        compiler_params=pltpu.CompilerParams(vmem_limit_bytes=mib * 2**20),
    )(*args)
    return out[0] if single else out


def sides(a, b):
    return jnp.concatenate([a, b], axis=1)


def pack_body(wg, wu, wd, out):
    hid = wd.shape[1] // NY
    tg = wg[...].astype(F32).T
    tu = wu[...].astype(F32).T
    td = wd[...].astype(F32).T
    parts = []
    for y in range(NY):
        s = slice(y * hid, (y + 1) * hid)
        parts.append(jnp.concatenate([tg[s], tu[s], td[s]], axis=0))
    out[0] = sides(parts[0], parts[2]).astype(BF)
    out[1] = sides(parts[1], parts[3]).astype(BF)


def spread_body(own, far, out):
    half = own.shape[2] // 2
    for i in range(2):
        o, f = own[i].astype(F32), far[i].astype(F32)
        low = sides(o[:, :half], f[:, :half]).astype(BF)
        high = sides(o[:, half:], f[:, half:]).astype(BF)
        for r in range(NR):
            out[r * NY + i] = low
            out[r * NY + i + 2] = high


def weights_into(wt, chunks, r, rows):
    half = chunks.shape[2] // 2
    for side in range(NQ):
        cut = slice(side * half, (side + 1) * half)
        wt[NQ * r + side] = jnp.concatenate(
            [chunks[r * NY + y][:rows, cut] for y in range(NY)], axis=1
        )


def near_x(side, r, zq, x_here):
    return (2 * ((side + zq) % NQ) + r // NC + NX - x_here) % NX


def layer_body(refs):
    mine, other, chunks_far = refs[:4], refs[4:8], refs[8]
    pieces_far, turned_far = refs[9:11]
    one, two, chunks, pieces, turned, wt, sems = refs[11:]
    core = lax.axis_index("c")
    x_here = lax.axis_index("x")
    zq = lax.axis_index("zq")
    hid = chunks.shape[1] // 3
    half = chunks.shape[2] // 2

    first = pltpu.make_async_copy(chunks_far, chunks, sems.at[8])
    first.start()
    loads = []
    for i in range(4):
        loads.append(pltpu.make_async_copy(mine[i], one.at[i], sems.at[i]))
        loads.append(pltpu.make_async_copy(other[i], two.at[i], sems.at[4 + i]))
    for c in loads:
        c.start()
    first.wait()
    for r in range(NR):
        weights_into(wt, chunks, r, 3 * hid)
    for c in loads:
        c.wait()

    def run(even, odd):
        def block(side, r, which):
            k = near_x(side, r, zq, x_here)
            part = even[:, k, which] if r % NC == 0 else odd[k, :, which]
            return part.reshape(NY * part.shape[1], part.shape[2])

        pre = None
        hid_grad = None
        for r in range(NR):
            for side in range(NQ):
                p = dot(wt[NQ * r + side, : 2 * hid, :], block(side, r, 0), NT)
                q = dot(wt[NQ * r + side, 2 * hid :, :], block(side, r, 1), NT)
                pre = p if pre is None else pre + p
                hid_grad = q if hid_grad is None else hid_grad + q
        gate = pre[:hid]
        up = pre[hid:]
        sig = jax.nn.sigmoid(gate)
        act = gate * sig
        hidden = (act * up).astype(BF)
        g_gate = hid_grad * up * sig * (1.0 + gate * (1.0 - sig))
        g_up = hid_grad * act
        g_both = jnp.concatenate([g_gate, g_up], axis=0)
        turned[...] = g_both.T.astype(BF)
        g_both = g_both.astype(BF)
        stores = [pltpu.make_async_copy(turned, turned_far, sems.at[4])]
        stores[0].start()
        for r in range(NR):
            made = []
            for side in range(NQ):
                pw = dot(g_both, block(side, r, 0), NN)
                pd = dot(hidden, block(side, r, 1), NN)
                made.append(jnp.concatenate([pw, pd], axis=0).astype(BF))
            for y in range(NY):
                s = slice(y * half, (y + 1) * half)
                pieces[r * NY + y] = sides(made[0][:, s], made[1][:, s])
            part = pl.ds(r * NY, NY)
            stores.append(pltpu.make_async_copy(pieces.at[part], pieces_far.at[part], sems.at[r]))
            stores[-1].start()
        for c in stores:
            c.wait()

    @pl.when(core == 0)
    def _():
        run(one, two)

    @pl.when(core == 1)
    def _():
        run(two, one)


def back_body(turned, chunks, keep, send, wt):
    core = lax.axis_index("c")
    x_here = lax.axis_index("x")
    zq = lax.axis_index("zq")
    rows = turned.shape[0] // NY
    for r in range(NR):
        weights_into(wt, chunks, r, wt.shape[1])

    def run(me):
        for r in range(NR):
            for side in range(NQ):
                k = near_x(side, r, zq, x_here)
                gi = dot(turned[...], wt[NQ * r + side], NN).astype(BF)
                ref = keep if r % NC == me else send
                for j in range(NY):
                    piece = gi[j * rows : (j + 1) * rows]
                    if r % NC == 0:
                        ref[k, j] = piece
                    else:
                        ref[j, k] = piece

    @pl.when(core == 0)
    def _():
        run(0)

    @pl.when(core == 1)
    def _():
        run(1)


def sum_body(pieces, out):
    zq = lax.axis_index("zq")
    half = pieces.shape[2] // 2

    def total(y):
        s = pieces[y].astype(F32)
        for r in range(1, NR):
            s = s + pieces[r * NY + y].astype(F32)
        return s

    for i in range(2):
        low, high = total(i), total(i + 2)
        own = sides(low[:, :half], high[:, :half]).astype(BF)
        far = sides(low[:, half:], high[:, half:]).astype(BF)
        for h in range(2):
            out[2 * h + zq, i] = own
            out[2 * h + 1 - zq, i] = far


def last_body(parts, gg, gu, gd):
    hid = parts.shape[2] // 3
    half = parts.shape[3] // 2
    s = []
    for i in range(2):
        v = parts[0, i].astype(F32)
        for q in range(1, 4):
            v = v + parts[q, i].astype(F32)
        s.append(v)
    by_y = [s[0][:, :half], s[1][:, :half], s[0][:, half:], s[1][:, half:]]
    gg[...] = jnp.concatenate([b[:hid] for b in by_y], axis=0).T
    gu[...] = jnp.concatenate([b[hid : 2 * hid] for b in by_y], axis=0).T
    gd[...] = jnp.concatenate([b[2 * hid :] for b in by_y], axis=0).T


def per_device(inputs, cotangent, gate_weight, up_weight, down_weight):
    S = jax.ShapeDtypeStruct
    rows_d, ff = gate_weight.shape
    hid = ff // NY
    rows, cols = inputs.shape

    packed = call(
        pack_body,
        (gate_weight, up_weight, down_weight.T),
        S((2, 3 * hid, 2 * rows_d), BF),
        60,
        far_in=3,
    )
    far = lax.ppermute(packed, "zq", [(0, 1), (1, 0)])
    chunks = call(spread_body, (packed, far), S((NR * NY, 3 * hid, 2 * rows_d), BF), 60, far_in=2)
    chunks = lax.all_to_all(chunks, ("zr", "y"), 0, 0, tiled=True)

    block = jnp.stack([inputs, cotangent])
    line = jnp.stack(line_gather(block, 0))
    mine = line_gather(line, 1)
    other = [swapped(m) for m in mine]

    tiles = S((4, 4, rows, cols), BF)
    turned = S((NY * rows, 2 * hid), BF)
    joint = (4, *mine[0].shape)
    made = [S(chunks.shape, BF), turned]
    far = pl.BlockSpec(memory_space=pltpu.HBM)
    shapes = (joint, joint, chunks.shape, chunks.shape, turned.shape)
    shapes += ((NQ * NR, 3 * hid, NY * rows_d),)
    pieces, turned = pl.pallas_call(
        lambda *refs: layer_body(refs),
        in_specs=[far] * 9,
        out_specs=[far] * 2,
        out_shape=made,
        scratch_shapes=[pltpu.VMEM(s, BF) for s in shapes] + [pltpu.SemaphoreType.DMA((9,))],
        compiler_params=pltpu.CompilerParams(vmem_limit_bytes=60 * 2**20),
        name="layer",
    )(*mine, *other, chunks)

    pieces = lax.all_to_all(pieces, ("zr", "y"), 0, 0, tiled=True)
    ring = call(sum_body, (pieces,), S((4, 2, 3 * hid, 2 * rows_d), BF))
    ring = lax.all_to_all(ring, ("zh", "zq"), 0, 0, tiled=True)
    g_gate, g_up, g_down = call(last_body, (ring,), [S((rows_d, ff), F32)] * 3)

    keep, send = call(
        back_body,
        (turned, chunks),
        [tiles, tiles],
        60,
        far_in=2,
        far_out=True,
        own=[pltpu.VMEM((NQ * NR, 2 * hid, NY * rows_d), BF)],
    )
    theirs = swapped(send)
    chip = (keep.astype(F32) + theirs.astype(F32)).astype(BF)
    part = line_sum(chip, 0)
    done = line_sum(part, 1)
    return (done, g_gate, g_up, g_down.T)


def solution(mesh):
    fine = Mesh(mesh.devices.reshape(2, NQ, NR, NY, NX, NC), ("zh", "zq", "zr", "y", "x", "c"))
    tok, fs, tp = ("zh", "zq", "zr", "y"), ("zq", "zr", "y"), ("x", "c")

    return jax.shard_map(
        per_device,
        mesh=fine,
        in_specs=(P(tok, tp), P(tok, tp), P(fs, tp), P(fs, tp), P(tp, fs)),
        out_specs=(P(tok, tp), P(fs, tp), P(fs, tp), P(tp, fs)),
        check_vma=False,
    )
```

```python
import jax
import jax.numpy as jnp
from jax import lax
from jax.experimental import pallas as pl
from jax.experimental.pallas import tpu as pltpu
from jax.sharding import Mesh, PartitionSpec as P


BF = jnp.bfloat16
F32 = jnp.float32
NQ, NR, NY, NX, NC = 2, 4, 4, 4, 2
PLANE = ("y", "x", "c")
VM = pl.BlockSpec(memory_space=pltpu.VMEM)
NN = ((1,), (0,))
NT = ((1,), (1,))


def swapped(value):
    return lax.ppermute(value, "c", [(0, 1), (1, 0)])


def moved(value, mask, x_core):
    pairs = []
    for y in range(NY):
        for x in range(NX):
            for c in range(NC):
                ty, tx = (y, x ^ mask) if c == x_core else (y ^ mask, x)
                pairs.append(((y * NX + x) * NC + c, (ty * NX + tx) * NC + c))
    return lax.ppermute(value, PLANE, pairs)


def line_double(value, x_core):
    two = jnp.stack([value, moved(value, 1, x_core)])
    return jnp.concatenate([two, moved(two, 2, x_core)], axis=0)


def line_gather(value, x_core):
    return [value] + [moved(value, m, x_core) for m in (1, 2, 3)]


def line_sum(value, x_core):
    total = value[0].astype(F32)
    for m in (1, 2, 3):
        total = total + moved(value[m], m, x_core).astype(F32)
    return total.astype(BF)


def dot(a, b, dims):
    return lax.dot_general(a, b, (dims, ((), ())), preferred_element_type=F32)


def call(body, args, shapes, mib=8, far_in=0, far_out=False, own=()):
    single = not isinstance(shapes, (list, tuple))
    shapes = [shapes] if single else list(shapes)
    n, m = len(args), len(shapes)
    loads, stores = far_in, m if far_out else 0

    def whole(*refs):
        ins, outs, rest = list(refs[:n]), list(refs[n : n + m]), refs[n + m :]
        mid = loads + stores
        near_in, near_out = rest[:loads], rest[loads:mid]
        held, rest = rest[mid : mid + len(own)], rest[mid + len(own) :]
        if loads:
            sems = rest[0]
            copies = [pltpu.make_async_copy(ins[i], near_in[i], sems.at[i]) for i in range(loads)]
            for c in copies:
                c.start()
            for c in copies:
                c.wait()
        body(*near_in, *ins[loads:], *(near_out if stores else outs), *held)
        if stores:
            sems = rest[-1]
            copies = [pltpu.make_async_copy(near_out[i], outs[i], sems.at[i]) for i in range(m)]
            for c in copies:
                c.start()
            for c in copies:
                c.wait()

    far = pl.BlockSpec(memory_space=pltpu.HBM)
    scratch = [pltpu.VMEM(a.shape, a.dtype) for a in args[:loads]]
    scratch += [pltpu.VMEM(a.shape, a.dtype) for a in shapes[:stores]]
    scratch += list(own)
    scratch += [pltpu.SemaphoreType.DMA((k,)) for k in (loads, stores) if k]
    out = pl.pallas_call(
        whole,
        in_specs=[far] * loads + [VM] * (n - loads),
        out_specs=[far if far_out else VM] * m,
        out_shape=shapes,
        scratch_shapes=scratch,
        compiler_params=pltpu.CompilerParams(vmem_limit_bytes=mib * 2**20),
    )(*args)
    return out[0] if single else out


def sides(a, b):
    return jnp.concatenate([a, b], axis=1)


def pack_body(wg, wu, wd, out):
    hid = wd.shape[1] // NY
    tg = wg[...].astype(F32).T
    tu = wu[...].astype(F32).T
    td = wd[...].astype(F32).T
    parts = []
    for y in range(NY):
        s = slice(y * hid, (y + 1) * hid)
        parts.append(jnp.concatenate([tg[s], tu[s], td[s]], axis=0))
    out[0] = sides(parts[0], parts[2]).astype(BF)
    out[1] = sides(parts[1], parts[3]).astype(BF)


def spread_body(own, far, out):
    half = own.shape[2] // 2
    for i in range(2):
        o, f = own[i].astype(F32), far[i].astype(F32)
        low = sides(o[:, :half], f[:, :half]).astype(BF)
        high = sides(o[:, half:], f[:, half:]).astype(BF)
        for r in range(NR):
            out[r * NY + i] = low
            out[r * NY + i + 2] = high


def weights_into(wt, chunks, r, rows):
    half = chunks.shape[2] // 2
    for side in range(NQ):
        cut = slice(side * half, (side + 1) * half)
        wt[NQ * r + side] = jnp.concatenate(
            [chunks[r * NY + y][:rows, cut] for y in range(NY)], axis=1
        )


def near_x(side, r, zq, x_here):
    return (2 * ((side + zq) % NQ) + r // NC) ^ x_here


def layer_body(refs):
    mine, other, chunks_far = refs[:4], refs[4:8], refs[8]
    pieces_far, turned_far = refs[9:11]
    one, two, chunks, pieces, turned, wt, sems = refs[11:]
    core = lax.axis_index("c")
    x_here = lax.axis_index("x")
    zq = lax.axis_index("zq")
    hid = chunks.shape[1] // 3
    half = chunks.shape[2] // 2

    first = pltpu.make_async_copy(chunks_far, chunks, sems.at[8])
    first.start()
    loads = []
    for i in range(4):
        loads.append(pltpu.make_async_copy(mine[i], one.at[i], sems.at[i]))
        loads.append(pltpu.make_async_copy(other[i], two.at[i], sems.at[4 + i]))
    for c in loads:
        c.start()
    first.wait()
    for r in range(NR):
        weights_into(wt, chunks, r, 3 * hid)
    for c in loads:
        c.wait()

    def run(even, odd):
        def block(side, r, which):
            k = near_x(side, r, zq, x_here)
            part = even[:, k, which] if r % NC == 0 else odd[k, :, which]
            return part.reshape(NY * part.shape[1], part.shape[2])

        pre = None
        hid_grad = None
        for r in range(NR):
            for side in range(NQ):
                p = dot(wt[NQ * r + side, : 2 * hid, :], block(side, r, 0), NT)
                q = dot(wt[NQ * r + side, 2 * hid :, :], block(side, r, 1), NT)
                pre = p if pre is None else pre + p
                hid_grad = q if hid_grad is None else hid_grad + q
        gate = pre[:hid]
        up = pre[hid:]
        sig = jax.nn.sigmoid(gate)
        act = gate * sig
        hidden = (act * up).astype(BF)
        g_gate = hid_grad * up * sig * (1.0 + gate * (1.0 - sig))
        g_up = hid_grad * act
        g_both = jnp.concatenate([g_gate, g_up], axis=0)
        turned[...] = g_both.T.astype(BF)
        g_both = g_both.astype(BF)
        stores = [pltpu.make_async_copy(turned, turned_far, sems.at[4])]
        stores[0].start()
        for r in range(NR):
            made = []
            for side in range(NQ):
                pw = dot(g_both, block(side, r, 0), NN)
                pd = dot(hidden, block(side, r, 1), NN)
                made.append(jnp.concatenate([pw, pd], axis=0).astype(BF))
            for y in range(NY):
                s = slice(y * half, (y + 1) * half)
                pieces[r * NY + y] = sides(made[0][:, s], made[1][:, s])
            part = pl.ds(r * NY, NY)
            stores.append(pltpu.make_async_copy(pieces.at[part], pieces_far.at[part], sems.at[r]))
            stores[-1].start()
        for c in stores:
            c.wait()

    @pl.when(core == 0)
    def _():
        run(one, two)

    @pl.when(core == 1)
    def _():
        run(two, one)


def back_body(turned, chunks, keep, send, wt):
    core = lax.axis_index("c")
    x_here = lax.axis_index("x")
    zq = lax.axis_index("zq")
    rows = turned.shape[0] // NY
    for r in range(NR):
        weights_into(wt, chunks, r, wt.shape[1])

    def run(me):
        for r in range(NR):
            for side in range(NQ):
                k = near_x(side, r, zq, x_here)
                gi = dot(turned[...], wt[NQ * r + side], NN).astype(BF)
                ref = keep if r % NC == me else send
                for j in range(NY):
                    piece = gi[j * rows : (j + 1) * rows]
                    if r % NC == 0:
                        ref[k, j] = piece
                    else:
                        ref[j, k] = piece

    @pl.when(core == 0)
    def _():
        run(0)

    @pl.when(core == 1)
    def _():
        run(1)


def sum_body(pieces, out):
    zq = lax.axis_index("zq")
    half = pieces.shape[2] // 2

    def total(y):
        s = pieces[y].astype(F32)
        for r in range(1, NR):
            s = s + pieces[r * NY + y].astype(F32)
        return s

    for i in range(2):
        low, high = total(i), total(i + 2)
        own = sides(low[:, :half], high[:, :half]).astype(BF)
        far = sides(low[:, half:], high[:, half:]).astype(BF)
        for h in range(2):
            out[2 * h + zq, i] = own
            out[2 * h + 1 - zq, i] = far


def last_body(parts, gg, gu, gd):
    hid = parts.shape[2] // 3
    half = parts.shape[3] // 2
    s = []
    for i in range(2):
        v = parts[0, i].astype(F32)
        for q in range(1, 4):
            v = v + parts[q, i].astype(F32)
        s.append(v)
    by_y = [s[0][:, :half], s[1][:, :half], s[0][:, half:], s[1][:, half:]]
    gg[...] = jnp.concatenate([b[:hid] for b in by_y], axis=0).T
    gu[...] = jnp.concatenate([b[hid : 2 * hid] for b in by_y], axis=0).T
    gd[...] = jnp.concatenate([b[2 * hid :] for b in by_y], axis=0).T


def per_device(inputs, cotangent, gate_weight, up_weight, down_weight):
    S = jax.ShapeDtypeStruct
    rows_d, ff = gate_weight.shape
    hid = ff // NY
    rows, cols = inputs.shape

    packed = call(
        pack_body,
        (gate_weight, up_weight, down_weight.T),
        S((2, 3 * hid, 2 * rows_d), BF),
        60,
        far_in=3,
    )
    far = lax.ppermute(packed, "zq", [(0, 1), (1, 0)])
    chunks = call(spread_body, (packed, far), S((NR * NY, 3 * hid, 2 * rows_d), BF))
    chunks = lax.all_to_all(chunks, ("zr", "y"), 0, 0, tiled=True)

    block = jnp.stack([inputs, cotangent])
    line = line_double(block, 0)
    mine = line_gather(line, 1)
    other = [swapped(m) for m in mine]

    tiles = S((4, 4, rows, cols), BF)
    turned = S((NY * rows, 2 * hid), BF)
    joint = (4, *mine[0].shape)
    made = [S(chunks.shape, BF), turned]
    far = pl.BlockSpec(memory_space=pltpu.HBM)
    shapes = (joint, joint, chunks.shape, chunks.shape, turned.shape)
    shapes += ((NQ * NR, 3 * hid, NY * rows_d),)
    pieces, turned = pl.pallas_call(
        lambda *refs: layer_body(refs),
        in_specs=[far] * 9,
        out_specs=[far] * 2,
        out_shape=made,
        scratch_shapes=[pltpu.VMEM(s, BF) for s in shapes] + [pltpu.SemaphoreType.DMA((9,))],
        compiler_params=pltpu.CompilerParams(vmem_limit_bytes=60 * 2**20),
        name="layer",
    )(*mine, *other, chunks)

    pieces = lax.all_to_all(pieces, ("zr", "y"), 0, 0, tiled=True)
    ring = call(sum_body, (pieces,), S((4, 2, 3 * hid, 2 * rows_d), BF))
    ring = lax.all_to_all(ring, ("zh", "zq"), 0, 0, tiled=True)
    g_gate, g_up, g_down = call(last_body, (ring,), [S((rows_d, ff), F32)] * 3)

    keep, send = call(
        back_body,
        (turned, chunks),
        [tiles, tiles],
        60,
        far_in=2,
        far_out=True,
        own=[pltpu.VMEM((NQ * NR, 2 * hid, NY * rows_d), BF)],
    )
    theirs = swapped(send)
    chip = (keep.astype(F32) + theirs.astype(F32)).astype(BF)
    part = line_sum(chip, 0)
    done = line_sum(part, 1)
    return (done, g_gate, g_up, g_down.T)


def solution(mesh):
    fine = Mesh(mesh.devices.reshape(2, NQ, NR, NY, NX, NC), ("zh", "zq", "zr", "y", "x", "c"))
    tok, fs, tp = ("zh", "zq", "zr", "y"), ("zq", "zr", "y"), ("x", "c")

    return jax.shard_map(
        per_device,
        mesh=fine,
        in_specs=(P(tok, tp), P(tok, tp), P(fs, tp), P(fs, tp), P(tp, fs)),
        out_specs=(P(tok, tp), P(fs, tp), P(fs, tp), P(tp, fs)),
        check_vma=False,
    )
```

```python
import jax
import jax.numpy as jnp
from jax import lax
from jax.experimental import pallas as pl
from jax.experimental.pallas import tpu as pltpu
from jax.sharding import Mesh, PartitionSpec as P


BF = jnp.bfloat16
F32 = jnp.float32
NQ, NR, NY, NX, NC = 2, 4, 4, 4, 2
PLANE = ("y", "x", "c")
VM = pl.BlockSpec(memory_space=pltpu.VMEM)
NN = ((1,), (0,))
NT = ((1,), (1,))


def swapped(value):
    return lax.ppermute(value, "c", [(0, 1), (1, 0)])


def moved(value, mask, x_core):
    pairs = []
    for y in range(NY):
        for x in range(NX):
            for c in range(NC):
                ty, tx = (y, x ^ mask) if c == x_core else (y ^ mask, x)
                pairs.append(((y * NX + x) * NC + c, (ty * NX + tx) * NC + c))
    return lax.ppermute(value, PLANE, pairs)


def line_double(value, x_core):
    two = jnp.stack([value, moved(value, 1, x_core)])
    return jnp.concatenate([two, moved(two, 2, x_core)], axis=0)


def line_gather(value, x_core):
    return [value] + [moved(value, m, x_core) for m in (1, 2, 3)]


def line_sum(value, x_core):
    total = value[0].astype(F32)
    for m in (1, 2, 3):
        total = total + moved(value[m], m, x_core).astype(F32)
    return total.astype(BF)


def dot(a, b, dims):
    return lax.dot_general(a, b, (dims, ((), ())), preferred_element_type=F32)


def call(body, args, shapes, mib=8, far_in=0, far_out=False, own=()):
    single = not isinstance(shapes, (list, tuple))
    shapes = [shapes] if single else list(shapes)
    n, m = len(args), len(shapes)
    loads, stores = far_in, m if far_out else 0

    def whole(*refs):
        ins, outs, rest = list(refs[:n]), list(refs[n : n + m]), refs[n + m :]
        mid = loads + stores
        near_in, near_out = rest[:loads], rest[loads:mid]
        held, rest = rest[mid : mid + len(own)], rest[mid + len(own) :]
        if loads:
            sems = rest[0]
            copies = [pltpu.make_async_copy(ins[i], near_in[i], sems.at[i]) for i in range(loads)]
            for c in copies:
                c.start()
            for c in copies:
                c.wait()
        body(*near_in, *ins[loads:], *(near_out if stores else outs), *held)
        if stores:
            sems = rest[-1]
            copies = [pltpu.make_async_copy(near_out[i], outs[i], sems.at[i]) for i in range(m)]
            for c in copies:
                c.start()
            for c in copies:
                c.wait()

    far = pl.BlockSpec(memory_space=pltpu.HBM)
    scratch = [pltpu.VMEM(a.shape, a.dtype) for a in args[:loads]]
    scratch += [pltpu.VMEM(a.shape, a.dtype) for a in shapes[:stores]]
    scratch += list(own)
    scratch += [pltpu.SemaphoreType.DMA((k,)) for k in (loads, stores) if k]
    out = pl.pallas_call(
        whole,
        in_specs=[far] * loads + [VM] * (n - loads),
        out_specs=[far if far_out else VM] * m,
        out_shape=shapes,
        scratch_shapes=scratch,
        compiler_params=pltpu.CompilerParams(vmem_limit_bytes=mib * 2**20),
    )(*args)
    return out[0] if single else out


def sides(a, b):
    return jnp.concatenate([a, b], axis=1)


def cut_of(n):
    return -(-n // 32) * 16


def pack_body(wg, wu, wd, out, every):
    hid = wd.shape[1] // NY
    cut = out.shape[1]
    tg = wg[...].astype(F32).T
    tu = wu[...].astype(F32).T
    td = wd[...].astype(F32).T
    for y in range(NY):
        s = slice(y * hid, (y + 1) * hid)
        part = jnp.concatenate([tg[s], tu[s], td[s]], axis=0)
        gap = jnp.zeros((2 * cut - part.shape[0], part.shape[1]), F32)
        low = jnp.concatenate([part[cut:], gap], axis=0)
        part = sides(part[:cut], low).astype(BF)
        out[y] = part
        for r in range(NR):
            every[r * NY + y] = part


def weights_into(wt, chunks, r, side, rows):
    n, width = chunks.shape[1:]
    half = width // 2

    def whole(chunk):
        if rows <= n:
            return chunk[:rows, :half]
        return jnp.concatenate([chunk[:, :half], chunk[: rows - n, half:]], axis=0)

    wt[NQ * r + side] = jnp.concatenate([whole(chunks[r * NY + y]) for y in range(NY)], axis=1)


def near_x(side, r, zq, x_here):
    return (2 * ((side + zq) % NQ) + r // NC) ^ x_here


def layer_body(refs):
    mine, other, chunks_far = refs[:4], refs[4:8], refs[8:10]
    pieces_far, turned_far = refs[10:12]
    one, two, near, far, pieces, turned, wt, sems = refs[12:]
    core = lax.axis_index("c")
    x_here = lax.axis_index("x")
    zq = lax.axis_index("zq")
    hid = wt.shape[1] // 3
    half = pieces.shape[2] // 2

    first = [
        pltpu.make_async_copy(chunks_far[i], v, sems.at[8 + i]) for i, v in enumerate((near, far))
    ]
    for c in first:
        c.start()
    loads = []
    for i in range(4):
        loads.append(pltpu.make_async_copy(mine[i], one.at[i], sems.at[i]))
        loads.append(pltpu.make_async_copy(other[i], two.at[i], sems.at[4 + i]))
    for c in loads:
        c.start()
    for side, v in enumerate((near, far)):
        first[side].wait()
        for r in range(NR):
            weights_into(wt, v, r, side, 3 * hid)
    for c in loads:
        c.wait()

    def run(even, odd):
        def block(side, r, which):
            k = near_x(side, r, zq, x_here)
            part = even[:, k, which] if r % NC == 0 else odd[k, :, which]
            return part.reshape(NY * part.shape[1], part.shape[2])

        pre = None
        hid_grad = None
        for r in range(NR):
            for side in range(NQ):
                p = dot(wt[NQ * r + side, : 2 * hid, :], block(side, r, 0), NT)
                q = dot(wt[NQ * r + side, 2 * hid :, :], block(side, r, 1), NT)
                pre = p if pre is None else pre + p
                hid_grad = q if hid_grad is None else hid_grad + q
        gate = pre[:hid]
        up = pre[hid:]
        sig = jax.nn.sigmoid(gate)
        act = gate * sig
        hidden = (act * up).astype(BF)
        g_gate = hid_grad * up * sig * (1.0 + gate * (1.0 - sig))
        g_up = hid_grad * act
        g_both = jnp.concatenate([g_gate, g_up], axis=0)
        turned[...] = g_both.T.astype(BF)
        g_both = g_both.astype(BF)
        stores = [pltpu.make_async_copy(turned, turned_far, sems.at[4])]
        stores[0].start()
        for r in range(NR):
            made = []
            for side in range(NQ):
                pw = dot(g_both, block(side, r, 0), NN)
                pd = dot(hidden, block(side, r, 1), NN)
                made.append(jnp.concatenate([pw, pd], axis=0).astype(BF))
            for y in range(NY):
                s = slice(y * half, (y + 1) * half)
                pieces[r * NY + y] = sides(made[0][:, s], made[1][:, s])
            part = pl.ds(r * NY, NY)
            stores.append(pltpu.make_async_copy(pieces.at[part], pieces_far.at[part], sems.at[r]))
            stores[-1].start()
        for c in stores:
            c.wait()

    @pl.when(core == 0)
    def _():
        run(one, two)

    @pl.when(core == 1)
    def _():
        run(two, one)


def back_body(turned, near, far, keep, send, wt):
    core = lax.axis_index("c")
    x_here = lax.axis_index("x")
    zq = lax.axis_index("zq")
    rows = turned.shape[0] // NY
    for side, v in enumerate((near, far)):
        for r in range(NR):
            weights_into(wt, v, r, side, wt.shape[1])

    def run(me):
        for r in range(NR):
            for side in range(NQ):
                k = near_x(side, r, zq, x_here)
                gi = dot(turned[...], wt[NQ * r + side], NN).astype(BF)
                ref = keep if r % NC == me else send
                for j in range(NY):
                    piece = gi[j * rows : (j + 1) * rows]
                    if r % NC == 0:
                        ref[k, j] = piece
                    else:
                        ref[j, k] = piece

    @pl.when(core == 0)
    def _():
        run(0)

    @pl.when(core == 1)
    def _():
        run(1)


def sum_body(pieces, out):
    zq = lax.axis_index("zq")
    half = pieces.shape[2] // 2

    def total(y):
        s = pieces[y].astype(F32)
        for r in range(1, NR):
            s = s + pieces[r * NY + y].astype(F32)
        return s

    for i in range(2):
        low, high = total(i), total(i + 2)
        own = sides(low[:, :half], high[:, :half]).astype(BF)
        far = sides(low[:, half:], high[:, half:]).astype(BF)
        for h in range(2):
            out[2 * h + zq, i] = own
            out[2 * h + 1 - zq, i] = far


def last_body(parts, gg, gu, gd):
    hid = parts.shape[2] // 3
    half = parts.shape[3] // 2
    s = []
    for i in range(2):
        v = parts[0, i].astype(F32)
        for q in range(1, 4):
            v = v + parts[q, i].astype(F32)
        s.append(v)
    by_y = [s[0][:, :half], s[1][:, :half], s[0][:, half:], s[1][:, half:]]
    gg[...] = jnp.concatenate([b[:hid] for b in by_y], axis=0).T
    gu[...] = jnp.concatenate([b[hid : 2 * hid] for b in by_y], axis=0).T
    gd[...] = jnp.concatenate([b[2 * hid :] for b in by_y], axis=0).T


def per_device(inputs, cotangent, gate_weight, up_weight, down_weight):
    S = jax.ShapeDtypeStruct
    rows_d, ff = gate_weight.shape
    hid = ff // NY
    rows, cols = inputs.shape

    cut = cut_of(3 * hid)
    packed, near = call(
        pack_body,
        (gate_weight, up_weight, down_weight.T),
        [S((NY, cut, 2 * rows_d), BF), S((NR * NY, cut, 2 * rows_d), BF)],
        60,
        far_in=3,
    )
    far = lax.ppermute(packed, "zq", [(0, 1), (1, 0)])
    near = lax.all_to_all(near, ("zr", "y"), 0, 0, tiled=True)
    far = jnp.broadcast_to(far[None], (NR, *far.shape)).reshape(near.shape)
    far = lax.all_to_all(far, ("zr", "y"), 0, 0, tiled=True)

    block = jnp.stack([inputs, cotangent])
    line = line_double(block, 0)
    mine = line_gather(line, 1)
    other = [swapped(m) for m in mine]

    tiles = S((4, 4, rows, cols), BF)
    turned = S((NY * rows, 2 * hid), BF)
    joint = (4, *mine[0].shape)
    out = (NR * NY, 3 * hid, NQ * rows_d)
    hbm = pl.BlockSpec(memory_space=pltpu.HBM)
    shapes = (joint, joint, near.shape, far.shape, out, turned.shape)
    shapes += ((NQ * NR, 3 * hid, NY * rows_d),)
    pieces, turned = pl.pallas_call(
        lambda *refs: layer_body(refs),
        in_specs=[hbm] * 10,
        out_specs=[hbm] * 2,
        out_shape=[S(out, BF), turned],
        scratch_shapes=[pltpu.VMEM(s, BF) for s in shapes] + [pltpu.SemaphoreType.DMA((10,))],
        compiler_params=pltpu.CompilerParams(vmem_limit_bytes=60 * 2**20),
        name="layer",
    )(*mine, *other, near, far)

    pieces = lax.all_to_all(pieces, ("zr", "y"), 0, 0, tiled=True)
    ring = call(sum_body, (pieces,), S((4, 2, 3 * hid, 2 * rows_d), BF))
    ring = lax.all_to_all(ring, ("zh", "zq"), 0, 0, tiled=True)
    g_gate, g_up, g_down = call(last_body, (ring,), [S((rows_d, ff), F32)] * 3)

    keep, send = call(
        back_body,
        (turned, near, far),
        [tiles, tiles],
        60,
        far_in=3,
        far_out=True,
        own=[pltpu.VMEM((NQ * NR, 2 * hid, NY * rows_d), BF)],
    )
    theirs = swapped(send)
    chip = (keep.astype(F32) + theirs.astype(F32)).astype(BF)
    part = line_sum(chip, 0)
    done = line_sum(part, 1)
    return (done, g_gate, g_up, g_down.T)


def solution(mesh):
    fine = Mesh(mesh.devices.reshape(2, NQ, NR, NY, NX, NC), ("zh", "zq", "zr", "y", "x", "c"))
    tok, fs, tp = ("zh", "zq", "zr", "y"), ("zq", "zr", "y"), ("x", "c")

    return jax.shard_map(
        per_device,
        mesh=fine,
        in_specs=(P(tok, tp), P(tok, tp), P(fs, tp), P(fs, tp), P(tp, fs)),
        out_specs=(P(tok, tp), P(fs, tp), P(fs, tp), P(tp, fs)),
        check_vma=False,
    )
```

```python
import jax
import jax.numpy as jnp
from jax import lax
from jax.experimental import pallas as pl
from jax.experimental.pallas import tpu as pltpu
from jax.sharding import Mesh, PartitionSpec as P


BF = jnp.bfloat16
F32 = jnp.float32
NQ, NR, NY, NX, NC = 2, 4, 4, 4, 2
PLANE = ("y", "x", "c")
VM = pl.BlockSpec(memory_space=pltpu.VMEM)
NN = ((1,), (0,))
NT = ((1,), (1,))


def swapped(value):
    return lax.ppermute(value, "c", [(0, 1), (1, 0)])


def moved(value, mask, x_core):
    pairs = []
    for y in range(NY):
        for x in range(NX):
            for c in range(NC):
                ty, tx = (y, x ^ mask) if c == x_core else (y ^ mask, x)
                pairs.append(((y * NX + x) * NC + c, (ty * NX + tx) * NC + c))
    return lax.ppermute(value, PLANE, pairs)


def line_gather(value, x_core):
    return [value] + [moved(value, m, x_core) for m in (1, 2, 3)]


def line_sum(value, x_core):
    total = value[0].astype(F32)
    for m in (1, 2, 3):
        total = total + moved(value[m], m, x_core).astype(F32)
    return total.astype(BF)


def dot(a, b, dims):
    return lax.dot_general(a, b, (dims, ((), ())), preferred_element_type=F32)


def call(body, args, shapes, mib=8, far_in=0, far_out=False, own=()):
    single = not isinstance(shapes, (list, tuple))
    shapes = [shapes] if single else list(shapes)
    n, m = len(args), len(shapes)
    loads, stores = far_in, m if far_out else 0

    def whole(*refs):
        ins, outs, rest = list(refs[:n]), list(refs[n : n + m]), refs[n + m :]
        mid = loads + stores
        near_in, near_out = rest[:loads], rest[loads:mid]
        held, rest = rest[mid : mid + len(own)], rest[mid + len(own) :]
        if loads:
            sems = rest[0]
            copies = [pltpu.make_async_copy(ins[i], near_in[i], sems.at[i]) for i in range(loads)]
            for c in copies:
                c.start()
            for c in copies:
                c.wait()
        body(*near_in, *ins[loads:], *(near_out if stores else outs), *held)
        if stores:
            sems = rest[-1]
            copies = [pltpu.make_async_copy(near_out[i], outs[i], sems.at[i]) for i in range(m)]
            for c in copies:
                c.start()
            for c in copies:
                c.wait()

    far = pl.BlockSpec(memory_space=pltpu.HBM)
    scratch = [pltpu.VMEM(a.shape, a.dtype) for a in args[:loads]]
    scratch += [pltpu.VMEM(a.shape, a.dtype) for a in shapes[:stores]]
    scratch += list(own)
    scratch += [pltpu.SemaphoreType.DMA((k,)) for k in (loads, stores) if k]
    out = pl.pallas_call(
        whole,
        in_specs=[far] * loads + [VM] * (n - loads),
        out_specs=[far if far_out else VM] * m,
        out_shape=shapes,
        scratch_shapes=scratch,
        compiler_params=pltpu.CompilerParams(vmem_limit_bytes=mib * 2**20),
    )(*args)
    return out[0] if single else out


def sides(a, b):
    return jnp.concatenate([a, b], axis=1)


def cut_of(n):
    return -(-n // 32) * 16


def pack_body(wg, wu, wd, out, every):
    hid = wd.shape[1] // NY
    cut = out.shape[1]
    tg = wg[...].astype(F32).T
    tu = wu[...].astype(F32).T
    td = wd[...].astype(F32).T
    for y in range(NY):
        s = slice(y * hid, (y + 1) * hid)
        part = jnp.concatenate([tg[s], tu[s], td[s]], axis=0)
        gap = jnp.zeros((2 * cut - part.shape[0], part.shape[1]), F32)
        low = jnp.concatenate([part[cut:], gap], axis=0)
        part = sides(part[:cut], low).astype(BF)
        out[y] = part
        for r in range(NR):
            every[r * NY + y] = part


def weights_into(wt, chunks, r, side, rows):
    n, width = chunks.shape[1:]
    half = width // 2

    def whole(chunk):
        if rows <= n:
            return chunk[:rows, :half]
        return jnp.concatenate([chunk[:, :half], chunk[: rows - n, half:]], axis=0)

    wt[NQ * r + side] = jnp.concatenate([whole(chunks[r * NY + y]) for y in range(NY)], axis=1)


def near_x(side, r, zq, x_here):
    return (2 * ((side + zq) % NQ) + r // NC) ^ x_here


def layer_body(refs):
    mine, other, chunks_far = refs[:4], refs[4:8], refs[8:10]
    pieces_far, turned_far = refs[10:12]
    one, two, near, far, pieces, turned, wt, sems = refs[12:]
    core = lax.axis_index("c")
    x_here = lax.axis_index("x")
    zq = lax.axis_index("zq")
    hid = wt.shape[1] // 3
    half = pieces.shape[2] // 2

    first = [
        pltpu.make_async_copy(chunks_far[i], v, sems.at[8 + i]) for i, v in enumerate((near, far))
    ]
    for c in first:
        c.start()
    loads = []
    for i in range(4):
        loads.append(pltpu.make_async_copy(mine[i], one.at[i], sems.at[i]))
        loads.append(pltpu.make_async_copy(other[i], two.at[i], sems.at[4 + i]))
    for c in loads:
        c.start()
    for side, v in enumerate((near, far)):
        first[side].wait()
        for r in range(NR):
            weights_into(wt, v, r, side, 3 * hid)
    for c in loads:
        c.wait()

    def run(even, odd):
        def block(side, r, which):
            k = near_x(side, r, zq, x_here)
            part = even[:, k, which] if r % NC == 0 else odd[k, :, which]
            return part.reshape(NY * part.shape[1], part.shape[2])

        pre = None
        hid_grad = None
        for r in range(NR):
            for side in range(NQ):
                p = dot(wt[NQ * r + side, : 2 * hid, :], block(side, r, 0), NT)
                q = dot(wt[NQ * r + side, 2 * hid :, :], block(side, r, 1), NT)
                pre = p if pre is None else pre + p
                hid_grad = q if hid_grad is None else hid_grad + q
        gate = pre[:hid]
        up = pre[hid:]
        sig = jax.nn.sigmoid(gate)
        act = gate * sig
        hidden = (act * up).astype(BF)
        g_gate = hid_grad * up * sig * (1.0 + gate * (1.0 - sig))
        g_up = hid_grad * act
        g_both = jnp.concatenate([g_gate, g_up], axis=0)
        turned[...] = g_both.T.astype(BF)
        g_both = g_both.astype(BF)
        stores = [pltpu.make_async_copy(turned, turned_far, sems.at[4])]
        stores[0].start()
        for r in range(NR):
            made = []
            for side in range(NQ):
                pw = dot(g_both, block(side, r, 0), NN)
                pd = dot(hidden, block(side, r, 1), NN)
                made.append(jnp.concatenate([pw, pd], axis=0).astype(BF))
            for y in range(NY):
                s = slice(y * half, (y + 1) * half)
                pieces[r * NY + y] = sides(made[0][:, s], made[1][:, s])
            part = pl.ds(r * NY, NY)
            stores.append(pltpu.make_async_copy(pieces.at[part], pieces_far.at[part], sems.at[r]))
            stores[-1].start()
        for c in stores:
            c.wait()

    @pl.when(core == 0)
    def _():
        run(one, two)

    @pl.when(core == 1)
    def _():
        run(two, one)


def back_body(turned, near, far, keep, send, wt):
    core = lax.axis_index("c")
    x_here = lax.axis_index("x")
    zq = lax.axis_index("zq")
    rows = turned.shape[0] // NY
    for side, v in enumerate((near, far)):
        for r in range(NR):
            weights_into(wt, v, r, side, wt.shape[1])

    def run(me):
        for r in range(NR):
            for side in range(NQ):
                k = near_x(side, r, zq, x_here)
                gi = dot(turned[...], wt[NQ * r + side], NN).astype(BF)
                ref = keep if r % NC == me else send
                for j in range(NY):
                    piece = gi[j * rows : (j + 1) * rows]
                    if r % NC == 0:
                        ref[k, j] = piece
                    else:
                        ref[j, k] = piece

    @pl.when(core == 0)
    def _():
        run(0)

    @pl.when(core == 1)
    def _():
        run(1)


def sum_body(pieces, out):
    zq = lax.axis_index("zq")
    half = pieces.shape[2] // 2

    def total(y):
        s = pieces[y].astype(F32)
        for r in range(1, NR):
            s = s + pieces[r * NY + y].astype(F32)
        return s

    for i in range(2):
        low, high = total(i), total(i + 2)
        own = sides(low[:, :half], high[:, :half]).astype(BF)
        far = sides(low[:, half:], high[:, half:]).astype(BF)
        for h in range(2):
            out[2 * h + zq, i] = own
            out[2 * h + 1 - zq, i] = far


def last_body(parts, gg, gu, gd):
    hid = parts.shape[2] // 3
    half = parts.shape[3] // 2
    s = []
    for i in range(2):
        v = parts[0, i].astype(F32)
        for q in range(1, 4):
            v = v + parts[q, i].astype(F32)
        s.append(v)
    by_y = [s[0][:, :half], s[1][:, :half], s[0][:, half:], s[1][:, half:]]
    gg[...] = jnp.concatenate([b[:hid] for b in by_y], axis=0).T
    gu[...] = jnp.concatenate([b[hid : 2 * hid] for b in by_y], axis=0).T
    gd[...] = jnp.concatenate([b[2 * hid :] for b in by_y], axis=0).T


def per_device(inputs, cotangent, gate_weight, up_weight, down_weight):
    S = jax.ShapeDtypeStruct
    rows_d, ff = gate_weight.shape
    hid = ff // NY
    rows, cols = inputs.shape

    cut = cut_of(3 * hid)
    packed, near = call(
        pack_body,
        (gate_weight, up_weight, down_weight.T),
        [S((NY, cut, 2 * rows_d), BF), S((NR * NY, cut, 2 * rows_d), BF)],
        60,
        far_in=3,
    )
    far = lax.ppermute(packed, "zq", [(0, 1), (1, 0)])
    near = lax.all_to_all(near, ("zr", "y"), 0, 0, tiled=True)
    far = jnp.broadcast_to(far[None], (NR, *far.shape)).reshape(near.shape)
    far = lax.all_to_all(far, ("zr", "y"), 0, 0, tiled=True)

    block = jnp.stack([inputs, cotangent])
    line = jnp.stack(line_gather(block, 0))
    mine = line_gather(line, 1)
    other = [swapped(m) for m in mine]

    tiles = S((4, 4, rows, cols), BF)
    turned = S((NY * rows, 2 * hid), BF)
    joint = (4, *mine[0].shape)
    out = (NR * NY, 3 * hid, NQ * rows_d)
    hbm = pl.BlockSpec(memory_space=pltpu.HBM)
    shapes = (joint, joint, near.shape, far.shape, out, turned.shape)
    shapes += ((NQ * NR, 3 * hid, NY * rows_d),)
    pieces, turned = pl.pallas_call(
        lambda *refs: layer_body(refs),
        in_specs=[hbm] * 10,
        out_specs=[hbm] * 2,
        out_shape=[S(out, BF), turned],
        scratch_shapes=[pltpu.VMEM(s, BF) for s in shapes] + [pltpu.SemaphoreType.DMA((10,))],
        compiler_params=pltpu.CompilerParams(vmem_limit_bytes=63 * 2**20),
        name="layer",
    )(*mine, *other, near, far)

    pieces = lax.all_to_all(pieces, ("zr", "y"), 0, 0, tiled=True)
    ring = call(sum_body, (pieces,), S((4, 2, 3 * hid, 2 * rows_d), BF))
    ring = lax.all_to_all(ring, ("zh", "zq"), 0, 0, tiled=True)
    g_gate, g_up, g_down = call(last_body, (ring,), [S((rows_d, ff), F32)] * 3)

    keep, send = call(
        back_body,
        (turned, near, far),
        [tiles, tiles],
        60,
        far_in=3,
        far_out=True,
        own=[pltpu.VMEM((NQ * NR, 2 * hid, NY * rows_d), BF)],
    )
    theirs = swapped(send)
    chip = (keep.astype(F32) + theirs.astype(F32)).astype(BF)
    part = line_sum(chip, 0)
    done = line_sum(part, 1)
    return (done, g_gate, g_up, g_down.T)


def solution(mesh):
    fine = Mesh(mesh.devices.reshape(2, NQ, NR, NY, NX, NC), ("zh", "zq", "zr", "y", "x", "c"))
    tok, fs, tp = ("zh", "zq", "zr", "y"), ("zq", "zr", "y"), ("x", "c")

    return jax.shard_map(
        per_device,
        mesh=fine,
        in_specs=(P(tok, tp), P(tok, tp), P(fs, tp), P(fs, tp), P(tp, fs)),
        out_specs=(P(tok, tp), P(fs, tp), P(fs, tp), P(tp, fs)),
        check_vma=False,
    )
```

```python
import jax
import jax.numpy as jnp
from jax import lax
from jax.experimental import pallas as pl
from jax.experimental.pallas import tpu as pltpu
from jax.sharding import Mesh, PartitionSpec as P


BF = jnp.bfloat16
F32 = jnp.float32
NQ, NR, NY, NX, NC = 2, 4, 4, 4, 2
PLANE = ("y", "x", "c")
VM = pl.BlockSpec(memory_space=pltpu.VMEM)
NN = ((1,), (0,))
NT = ((1,), (1,))


def swapped(value):
    return lax.ppermute(value, "c", [(0, 1), (1, 0)])


def moved(value, mask, x_core):
    pairs = []
    for y in range(NY):
        for x in range(NX):
            for c in range(NC):
                ty, tx = (y, x ^ mask) if c == x_core else (y ^ mask, x)
                pairs.append(((y * NX + x) * NC + c, (ty * NX + tx) * NC + c))
    return lax.ppermute(value, PLANE, pairs)


def line_gather(value, x_core):
    return [value] + [moved(value, m, x_core) for m in (1, 2, 3)]


def line_sum(value, x_core):
    total = value[0].astype(F32)
    for m in (1, 2, 3):
        total = total + moved(value[m], m, x_core).astype(F32)
    return total.astype(BF)


def dot(a, b, dims):
    return lax.dot_general(a, b, (dims, ((), ())), preferred_element_type=F32)


def call(body, args, shapes, mib=8, far_in=0, far_out=False, own=()):
    single = not isinstance(shapes, (list, tuple))
    shapes = [shapes] if single else list(shapes)
    n, m = len(args), len(shapes)
    loads, stores = far_in, m if far_out else 0

    def whole(*refs):
        ins, outs, rest = list(refs[:n]), list(refs[n : n + m]), refs[n + m :]
        mid = loads + stores
        near_in, near_out = rest[:loads], rest[loads:mid]
        held, rest = rest[mid : mid + len(own)], rest[mid + len(own) :]
        if loads:
            sems = rest[0]
            copies = [pltpu.make_async_copy(ins[i], near_in[i], sems.at[i]) for i in range(loads)]
            for c in copies:
                c.start()
            for c in copies:
                c.wait()
        body(*near_in, *ins[loads:], *(near_out if stores else outs), *held)
        if stores:
            sems = rest[-1]
            copies = [pltpu.make_async_copy(near_out[i], outs[i], sems.at[i]) for i in range(m)]
            for c in copies:
                c.start()
            for c in copies:
                c.wait()

    far = pl.BlockSpec(memory_space=pltpu.HBM)
    scratch = [pltpu.VMEM(a.shape, a.dtype) for a in args[:loads]]
    scratch += [pltpu.VMEM(a.shape, a.dtype) for a in shapes[:stores]]
    scratch += list(own)
    scratch += [pltpu.SemaphoreType.DMA((k,)) for k in (loads, stores) if k]
    out = pl.pallas_call(
        whole,
        in_specs=[far] * loads + [VM] * (n - loads),
        out_specs=[far if far_out else VM] * m,
        out_shape=shapes,
        scratch_shapes=scratch,
        compiler_params=pltpu.CompilerParams(vmem_limit_bytes=mib * 2**20),
    )(*args)
    return out[0] if single else out


def sides(a, b):
    return jnp.concatenate([a, b], axis=1)


def cut_of(n):
    return -(-n // 32) * 16


def pack_body(wg, wu, wd, out, every):
    hid = wd.shape[1] // NY
    cut = out.shape[1]
    tg = wg[...].astype(F32).T
    tu = wu[...].astype(F32).T
    td = wd[...].astype(F32).T
    for y in range(NY):
        s = slice(y * hid, (y + 1) * hid)
        part = jnp.concatenate([tg[s], tu[s], td[s]], axis=0)
        gap = jnp.zeros((2 * cut - part.shape[0], part.shape[1]), F32)
        low = jnp.concatenate([part[cut:], gap], axis=0)
        part = sides(part[:cut], low).astype(BF)
        out[y] = part
        for r in range(NR):
            every[r * NY + y] = part


def weights_into(wt, chunks, r, side, rows):
    n, width = chunks.shape[1:]
    half = width // 2

    def whole(chunk):
        if rows <= n:
            return chunk[:rows, :half]
        return jnp.concatenate([chunk[:, :half], chunk[: rows - n, half:]], axis=0)

    wt[NQ * r + side] = jnp.concatenate([whole(chunks[r * NY + y]) for y in range(NY)], axis=1)


def near_x(side, r, zq, x_here):
    return (2 * ((side + zq) % NQ) + r // NC) ^ x_here


def layer_body(refs):
    mine, other, chunks_far = refs[:4], refs[4:8], refs[8:10]
    pieces_far, turned_far = refs[10:12]
    one, two, near, far, pieces, turned, wt, sems = refs[12:]
    core = lax.axis_index("c")
    x_here = lax.axis_index("x")
    zq = lax.axis_index("zq")
    hid = wt.shape[1] // 3
    half = pieces.shape[2] // 2

    first = [
        pltpu.make_async_copy(chunks_far[i], v, sems.at[8 + i]) for i, v in enumerate((near, far))
    ]
    for c in first:
        c.start()
    loads = []
    for i in range(4):
        loads.append(pltpu.make_async_copy(mine[i], one.at[i], sems.at[i]))
        loads.append(pltpu.make_async_copy(other[i], two.at[i], sems.at[4 + i]))
    for c in loads:
        c.start()
    for side, v in enumerate((near, far)):
        first[side].wait()
        for r in range(NR):
            weights_into(wt, v, r, side, 3 * hid)
    for c in loads:
        c.wait()

    def run(even, odd):
        def block(side, r, which):
            k = near_x(side, r, zq, x_here)
            part = even[:, k, which] if r % NC == 0 else odd[k, :, which]
            return part.reshape(NY * part.shape[1], part.shape[2])

        pre = None
        hid_grad = None
        for r in range(NR):
            for side in range(NQ):
                p = dot(wt[NQ * r + side, : 2 * hid, :], block(side, r, 0), NT)
                q = dot(wt[NQ * r + side, 2 * hid :, :], block(side, r, 1), NT)
                pre = p if pre is None else pre + p
                hid_grad = q if hid_grad is None else hid_grad + q
        gate = pre[:hid]
        up = pre[hid:]
        sig = jax.nn.sigmoid(gate)
        act = gate * sig
        hidden = (act * up).astype(BF)
        g_gate = hid_grad * up * sig * (1.0 + gate * (1.0 - sig))
        g_up = hid_grad * act
        g_both = jnp.concatenate([g_gate, g_up], axis=0)
        turned[...] = g_both.T.astype(BF)
        g_both = g_both.astype(BF)
        stores = [pltpu.make_async_copy(turned, turned_far, sems.at[4])]
        stores[0].start()
        for r in range(NR):
            made = []
            for side in range(NQ):
                pw = dot(g_both, block(side, r, 0), NN)
                pd = dot(hidden, block(side, r, 1), NN)
                made.append(jnp.concatenate([pw, pd], axis=0).astype(BF))
            for y in range(NY):
                s = slice(y * half, (y + 1) * half)
                pieces[r * NY + y] = sides(made[0][:, s], made[1][:, s])
            part = pl.ds(r * NY, NY)
            stores.append(pltpu.make_async_copy(pieces.at[part], pieces_far.at[part], sems.at[r]))
            stores[-1].start()
        for c in stores:
            c.wait()

    @pl.when(core == 0)
    def _():
        run(one, two)

    @pl.when(core == 1)
    def _():
        run(two, one)


def back_body(turned, near, far, keep, send, wt):
    core = lax.axis_index("c")
    x_here = lax.axis_index("x")
    zq = lax.axis_index("zq")
    rows = turned.shape[0] // NY
    for side, v in enumerate((near, far)):
        for r in range(NR):
            weights_into(wt, v, r, side, wt.shape[1])

    def run(me):
        for r in range(NR):
            for side in range(NQ):
                k = near_x(side, r, zq, x_here)
                gi = dot(turned[...], wt[NQ * r + side], NN).astype(BF)
                ref = keep if r % NC == me else send
                for j in range(NY):
                    piece = gi[j * rows : (j + 1) * rows]
                    if r % NC == 0:
                        ref[k, j] = piece
                    else:
                        ref[j, k] = piece

    @pl.when(core == 0)
    def _():
        run(0)

    @pl.when(core == 1)
    def _():
        run(1)


def sum_body(pieces, out):
    zq = lax.axis_index("zq")
    half = pieces.shape[2] // 2

    def total(y):
        s = pieces[y].astype(F32)
        for r in range(1, NR):
            s = s + pieces[r * NY + y].astype(F32)
        return s

    for i in range(2):
        low, high = total(i), total(i + 2)
        own = sides(low[:, :half], high[:, :half]).astype(BF)
        far = sides(low[:, half:], high[:, half:]).astype(BF)
        for h in range(2):
            out[2 * h + zq, i] = own
            out[2 * h + 1 - zq, i] = far


def last_body(parts, gg, gu, gd):
    hid = parts.shape[2] // 3
    half = parts.shape[3] // 2
    s = []
    for i in range(2):
        v = parts[0, i].astype(F32)
        for q in range(1, 4):
            v = v + parts[q, i].astype(F32)
        s.append(v)
    by_y = [s[0][:, :half], s[1][:, :half], s[0][:, half:], s[1][:, half:]]
    gg[...] = jnp.concatenate([b[:hid] for b in by_y], axis=0).T
    gu[...] = jnp.concatenate([b[hid : 2 * hid] for b in by_y], axis=0).T
    gd[...] = jnp.concatenate([b[2 * hid :] for b in by_y], axis=0).T


def per_device(inputs, cotangent, gate_weight, up_weight, down_weight):
    S = jax.ShapeDtypeStruct
    rows_d, ff = gate_weight.shape
    hid = ff // NY
    rows, cols = inputs.shape

    cut = cut_of(3 * hid)
    packed, near = call(
        pack_body,
        (gate_weight, up_weight, down_weight.T),
        [S((NY, cut, 2 * rows_d), BF), S((NR * NY, cut, 2 * rows_d), BF)],
        60,
        far_in=3,
    )
    far = lax.ppermute(packed, "zq", [(0, 1), (1, 0)])
    near = lax.all_to_all(near, ("zr", "y"), 0, 0, tiled=True)
    far = jnp.broadcast_to(far[None], (NR, *far.shape)).reshape(near.shape)
    far = lax.all_to_all(far, ("zr", "y"), 0, 0, tiled=True)

    block = jnp.stack([inputs, cotangent])
    line = jnp.stack(line_gather(block, 0))
    other = [swapped(line)]
    mine = [line]
    for m in (1, 2, 3):
        mine.append(moved(line, m, 1))
        other.append(swapped(mine[-1]))

    tiles = S((4, 4, rows, cols), BF)
    turned = S((NY * rows, 2 * hid), BF)
    joint = (4, *mine[0].shape)
    out = (NR * NY, 3 * hid, NQ * rows_d)
    hbm = pl.BlockSpec(memory_space=pltpu.HBM)
    shapes = (joint, joint, near.shape, far.shape, out, turned.shape)
    shapes += ((NQ * NR, 3 * hid, NY * rows_d),)
    pieces, turned = pl.pallas_call(
        lambda *refs: layer_body(refs),
        in_specs=[hbm] * 10,
        out_specs=[hbm] * 2,
        out_shape=[S(out, BF), turned],
        scratch_shapes=[pltpu.VMEM(s, BF) for s in shapes] + [pltpu.SemaphoreType.DMA((10,))],
        compiler_params=pltpu.CompilerParams(vmem_limit_bytes=63 * 2**20),
        name="layer",
    )(*mine, *other, near, far)

    pieces = lax.all_to_all(pieces, ("zr", "y"), 0, 0, tiled=True)
    ring = call(sum_body, (pieces,), S((4, 2, 3 * hid, 2 * rows_d), BF))
    ring = lax.all_to_all(ring, ("zh", "zq"), 0, 0, tiled=True)
    g_gate, g_up, g_down = call(last_body, (ring,), [S((rows_d, ff), F32)] * 3)

    keep, send = call(
        back_body,
        (turned, near, far),
        [tiles, tiles],
        60,
        far_in=3,
        far_out=True,
        own=[pltpu.VMEM((NQ * NR, 2 * hid, NY * rows_d), BF)],
    )
    theirs = swapped(send)
    chip = (keep.astype(F32) + theirs.astype(F32)).astype(BF)
    part = line_sum(chip, 0)
    done = line_sum(part, 1)
    return (done, g_gate, g_up, g_down.T)


def solution(mesh):
    fine = Mesh(mesh.devices.reshape(2, NQ, NR, NY, NX, NC), ("zh", "zq", "zr", "y", "x", "c"))
    tok, fs, tp = ("zh", "zq", "zr", "y"), ("zq", "zr", "y"), ("x", "c")

    return jax.shard_map(
        per_device,
        mesh=fine,
        in_specs=(P(tok, tp), P(tok, tp), P(fs, tp), P(fs, tp), P(tp, fs)),
        out_specs=(P(tok, tp), P(fs, tp), P(fs, tp), P(tp, fs)),
        check_vma=False,
    )
```
